32 devices in a mesh: ep: 16 (over z, y, x), tp: 2 (over core).
Axes of the slice: x: 2, y: 2, z: 4, core: 2. Of those that a mesh axis runs over, the one named last changes fastest.
Arguments:
- tokens: bfloat16 [256, 2048], P('ep'), may hold values from -6 to 6
- lengths: int32 [256], P('ep'), may hold values from 1024 to 8191
- prior_state: float32 [256, 16, 64, 64], P('ep', 'tp'), may hold values from -2 to 2
- mix_gain: float32 [2048], replicated, may hold values from 0.1 to 1.9
- post_gain: float32 [2048], replicated, may hold values from 0.1 to 1.9
- ffn_gain: float32 [2048], replicated, may hold values from 0.1 to 1.9
- out_gain: float32 [2048], replicated, may hold values from 0.1 to 1.9
- query_weight: bfloat16 [2048, 1024], P('ep', 'tp'), may hold values from -0.125 to 0.125
- key_weight: bfloat16 [2048, 1024], P('ep', 'tp'), may hold values from -0.125 to 0.125
- value_weight: bfloat16 [2048, 1024], P('ep', 'tp'), may hold values from -0.125 to 0.125
- gate_weight: bfloat16 [2048, 1024], P('ep', 'tp'), may hold values from -0.125 to 0.125
- out_weight: bfloat16 [1024, 2048], P('tp', 'ep'), may hold values from -0.1875 to 0.1875
- routes: int32 [256, 6], P('ep'), may hold values from 0 to 15, all different within a row; in each aligned block of 16 rows (0 to 15, 16 to 31, ...) at most 8 rows name the same one
- route_gates: float32 [256, 6], P('ep'), may hold values from 0.1 to 0.9
- expert_gate: bfloat16 [16, 2048, 512], P('ep', None, 'tp'), may hold values from -0.125 to 0.125
- expert_up: bfloat16 [16, 2048, 512], P('ep', None, 'tp'), may hold values from -0.125 to 0.125
- expert_down: bfloat16 [16, 512, 2048], P('ep', 'tp'), may hold values from -0.25 to 0.25
- shared_gate: bfloat16 [2048, 512], P(None, 'tp'), may hold values from -0.125 to 0.125
- shared_up: bfloat16 [2048, 512], P(None, 'tp'), may hold values from -0.125 to 0.125
- shared_down: bfloat16 [512, 2048], P('tp'), may hold values from -0.25 to 0.25
Outputs:
- result: bfloat16 [256, 2048], P('ep')
- new_state: float32 [256, 16, 64, 64], P('ep', 'tp')
The draws below stay inside these ranges and needn't reach their ends.
Inputs may be any that keep to these rules, and one draw needn't show every extreme that they name: `routes`: each row names 6 different experts. In the rows of one device (aligned blocks of 16 rows) no expert is named more than 8 times, and in every draw some expert is named exactly 8 times in some block.
All inputs are finite; a program needn't handle non-finite values.
Results may differ from the reference program's by a relative error of at most 0.02.
Values may be sent and summed in bfloat16 or wider, within the bound.
A program may use at most 128 MiB of HBM per device.

```python
import math
import jax
import jax.numpy as jnp
import numpy as np
from jax import lax

D = 2048
HEAD = 64
HEADS = 16
RW = 1024
FE = 512
FS = 512
TOPK = 6
SEQ_DEV = 16
TOKENS = 256
EXPERTS = 16
CAP = 8
N_EP = 16
N_TP = 2


def with_ends(values, rng, least, top_value):
    place = [jax.random.randint(jax.random.fold_in(rng, axis), (), 0, length) for axis, length in enumerate(values.shape)]
    longest = values.shape.index(max(values.shape))
    beside = place[:longest] + [(place[longest] + 1) % values.shape[longest]] + place[longest + 1:]
    return values.at[tuple(place)].set(least).at[tuple(beside)].set(top_value)


def block_levels(key, extent, pieces, least, top_value):
    loudness = 1.0
    for position, shards_of in pieces:
        draws = jax.random.uniform(jax.random.fold_in(jax.random.fold_in(key, 6), position), (shards_of,), jnp.float32, least / len(pieces), top_value / len(pieces))
        loudness = loudness * jnp.repeat(jnp.exp(draws), extent[position] // shards_of).reshape((-1,) + (1,) * (len(extent) - 1 - position))
    return loudness


def assign_block(rng, own, number, rows, amount, top, reach, lean):
    sequence = jax.random.permutation(rng, amount)
    crowded, common = portions_of(amount, rows * top, reach, lean, True), portions_of(amount, rows * top, reach, lean, False)
    places = jnp.arange(amount)

    def named(sizes, offset_by):
        used = int((sizes > 0).sum())
        fixed = max(1, used // 4)
        passed = fixed + (places - fixed + offset_by * (used - fixed)) % max(1, amount - fixed)
        return jnp.zeros((amount,), jnp.int32).at[sequence[jnp.where(places < fixed, places, passed)]].set(jnp.asarray(sizes, jnp.int32))

    sizes = jnp.where(number % 4 == 0, named(crowded, number // 4), named(common, number - number // 4 - 1))
    mixed = jax.random.permutation(jax.random.fold_in(own, 3), amount)
    source_of, receiver = mixed[0:amount // 2 * 2:2], mixed[1:amount // 2 * 2:2]
    room = jnp.minimum(sizes[source_of] - 1, reach - sizes[receiver]) // 2
    room = jnp.where((source_of == sequence[0]) | (receiver == sequence[0]) | (sizes[receiver] == 0), 0, jnp.maximum(room, 0))
    passed = jax.random.randint(jax.random.fold_in(own, 4), (amount // 2,), 0, 1 << 20) % (room + 1)
    sizes = sizes.at[source_of].add(-passed).at[receiver].add(passed)
    members = jnp.searchsorted(jnp.cumsum(sizes), jnp.arange(rows * top), side="right").astype(jnp.int32)
    table = members.reshape(top, rows).T
    table = table[jax.random.permutation(jax.random.fold_in(own, 1), rows)]
    offset_by = jax.random.randint(jax.random.fold_in(own, 2), (rows, 1), 0, top)
    return jnp.take_along_axis(table, (jnp.arange(top)[None, :] + offset_by) % top, axis=1)


def portions_of(number_of, total, most, lean, full):
    weights = [(1 << 20) // math.isqrt(rank ** lean) + 1 for rank in range(1, number_of + 1)]
    largest = most if full else min(most, max(-(-total // number_of), total * weights[0] // sum(weights)))
    least = 1 if total - largest >= number_of - 1 else 0
    counts, rest = [largest] + [least] * (number_of - 1), total - largest - least * (number_of - 1)
    while rest > 0:
        movable = [i for i in range(1, number_of) if counts[i] < largest] or [i for i in range(1, number_of) if counts[i] < most]
        pool, budget = sum([weights[i] for i in movable]), rest
        for i in movable:
            extra = min(most - counts[i], max(1, budget * weights[i] // pool), rest)
            counts[i] = counts[i] + extra
            rest = rest - extra
    return np.array(counts)


def bell_draw(key, dims, spread, most, cuts=(), kind=jnp.bfloat16):
    array = spread * jax.random.normal(key, dims, jnp.float32)
    if cuts:
        array = array * block_levels(key, dims, cuts, -0.22, 0.18)
    return jnp.clip(array, -most, most).astype(kind)


def setup_inputs(seed: int = 0) -> dict:
    keys = jax.random.split(jax.random.key(seed), 21)
    tokens = bell_draw(keys[0], (TOKENS, D), 1.0, 6.0, ((0, 16),))
    lengths = with_ends(jax.random.randint(keys[1], (TOKENS,), 1024, 8192), jax.random.fold_in(keys[1], 1), 1024, 8191).astype(jnp.int32)
    prior_state = bell_draw(keys[2], (TOKENS, HEADS, HEAD, HEAD), 0.15, 2.0, ((0, 16), (1, 2)), jnp.float32)
    mix_gain = jnp.clip(1.0 + 0.18 * jax.random.normal(keys[3], (D,), jnp.float32), 0.1, 1.9)
    post_gain = jnp.clip(1.0 + 0.18 * jax.random.normal(keys[4], (D,), jnp.float32), 0.1, 1.9)
    ffn_gain = jnp.clip(1.0 + 0.18 * jax.random.normal(keys[5], (D,), jnp.float32), 0.1, 1.9)
    out_gain = jnp.clip(1.0 + 0.18 * jax.random.normal(keys[6], (D,), jnp.float32), 0.1, 1.9)
    query_weight = bell_draw(keys[7], (D, RW), D ** -0.5, 0.125, ((0, 16), (1, 2)))
    key_weight = bell_draw(keys[8], (D, RW), D ** -0.5, 0.125, ((0, 16), (1, 2)))
    value_weight = bell_draw(keys[9], (D, RW), D ** -0.5, 0.125, ((0, 16), (1, 2)))
    gate_weight = bell_draw(keys[10], (D, RW), D ** -0.5, 0.125, ((0, 16), (1, 2)))
    out_weight = bell_draw(keys[11], (RW, D), RW ** -0.5, 0.1875, ((0, 2), (1, 16)))
    routes_keys = jax.random.split(jax.random.fold_in(keys[12], 1), TOKENS // SEQ_DEV)
    routes_turns = jax.random.permutation(jax.random.fold_in(keys[12], 3), TOKENS // SEQ_DEV)
    routes = jax.vmap(lambda own, number: assign_block(jax.random.fold_in(keys[12], 2), own, number, SEQ_DEV, EXPERTS, TOPK, CAP, 2))(routes_keys, routes_turns).reshape((TOKENS, TOPK))
    route_gates = jnp.clip(0.1 + 0.79999997 * jax.random.uniform(keys[13], (TOKENS, TOPK), jnp.float32) ** block_levels(keys[13], (TOKENS, TOPK), ((0, 16),), -0.2, 0.2), 0.1, 0.9)
    expert_gate = bell_draw(keys[14], (EXPERTS, D, FE), D ** -0.5, 0.125, ((0, 16), (2, 2)))
    expert_up = bell_draw(keys[15], (EXPERTS, D, FE), D ** -0.5, 0.125, ((0, 16), (2, 2)))
    expert_down = bell_draw(keys[16], (EXPERTS, FE, D), FE ** -0.5, 0.25, ((0, 16), (1, 2)))
    shared_gate = bell_draw(keys[17], (D, FS), D ** -0.5, 0.125, ((1, 2),))
    shared_up = bell_draw(keys[18], (D, FS), D ** -0.5, 0.125, ((1, 2),))
    shared_down = bell_draw(keys[19], (FS, D), FS ** -0.5, 0.25, ((0, 2),))
    return {"tokens": tokens, "lengths": lengths, "prior_state": prior_state, "mix_gain": mix_gain, "post_gain": post_gain, "ffn_gain": ffn_gain, "out_gain": out_gain, "query_weight": query_weight, "key_weight": key_weight, "value_weight": value_weight, "gate_weight": gate_weight, "out_weight": out_weight, "routes": routes, "route_gates": route_gates, "expert_gate": expert_gate, "expert_up": expert_up, "expert_down": expert_down, "shared_gate": shared_gate, "shared_up": shared_up, "shared_down": shared_down}


EPS = 1e-06
THETA = 10000.0

def rounded(values):
    return lax.optimization_barrier(values.astype(jnp.bfloat16)).astype(jnp.float32)

def scaled_rows(values, gain_row):
    widened = values.astype(jnp.float32)
    return widened * lax.rsqrt(lax.optimization_barrier(jnp.mean(widened * widened, axis=-1, keepdims=True)) + EPS) * gain_row.astype(jnp.float32)

def rotate(vectors, lengths):
    half_dim = vectors.shape[-1] // 2
    frequency = THETA ** (-jnp.arange(half_dim, dtype=jnp.float32) / half_dim)
    angles = lengths.astype(jnp.float32)[:, None] * frequency[None, :]
    cosine = jnp.cos(angles)[:, None, :]
    sine_part = jnp.sin(angles)[:, None, :]
    leading = vectors[..., :half_dim]
    trailing = vectors[..., half_dim:]
    return jnp.concatenate([leading * cosine - trailing * sine_part, trailing * cosine + leading * sine_part], axis=-1)

def decay_table(head_count):
    head_order = jnp.arange(head_count, dtype=jnp.float32)
    return 1.0 - jnp.exp2(-5.0 - 7.0 * head_order / (head_count - 1))

def retain(queries, keys_new, values, out_gate, prior_state, lengths, decays):
    seq_count = queries.shape[0]
    head_count = decays.shape[0]
    layout = (seq_count, head_count, HEAD)
    rot_query = rotate(queries.astype(jnp.float32).reshape(layout), lengths)
    rot_key = rotate(keys_new.astype(jnp.float32).reshape(layout), lengths) * HEAD ** (-0.5)
    wide_values = values.astype(jnp.float32).reshape(layout)
    from_state = jnp.einsum('shd,shde->she', rot_query, prior_state, precision=lax.Precision.HIGHEST)
    self_term = lax.optimization_barrier(jnp.sum(rot_query * rot_key, axis=-1, keepdims=True))
    read_out = decays[None, :, None] * from_state + self_term * wide_values
    new_state = decays[None, :, None, None] * prior_state + rot_key[..., :, None] * wide_values[..., None, :]
    normed = read_out * lax.rsqrt(lax.optimization_barrier(jnp.mean(read_out * read_out, axis=-1, keepdims=True)) + EPS)
    gated_rows = normed.reshape(seq_count, head_count * HEAD) * jax.nn.silu(out_gate.astype(jnp.float32))
    return (gated_rows.astype(jnp.bfloat16), new_state)

def swiglu_split(inputs, w_gate, w_up, w_down):
    part_width = w_gate.shape[1] // N_TP
    running = jnp.zeros((inputs.shape[0], w_down.shape[1]), jnp.float32)
    for portion in range(N_TP):
        lower_row = portion * part_width
        gate_cols = jnp.dot(inputs, w_gate[:, lower_row:lower_row + part_width], preferred_element_type=jnp.float32)
        up_cols = jnp.dot(inputs, w_up[:, lower_row:lower_row + part_width], preferred_element_type=jnp.float32)
        hidden = (jax.nn.silu(gate_cols) * up_cols).astype(jnp.bfloat16)
        running = running + rounded(jnp.dot(hidden, w_down[lower_row:lower_row + part_width, :], preferred_element_type=jnp.float32))
    return running.astype(jnp.bfloat16)

def reference(tokens, lengths, prior_state, mix_gain, post_gain, ffn_gain, out_gain, query_weight, key_weight, value_weight, gate_weight, out_weight, routes, route_gates, expert_gate, expert_up, expert_down, shared_gate, shared_up, shared_down):
    normed = scaled_rows(tokens, mix_gain).astype(jnp.bfloat16)

    def project(weight_matrix):
        return jnp.dot(normed, weight_matrix, preferred_element_type=jnp.float32).astype(jnp.bfloat16)
    retained, new_state = retain(project(query_weight), project(key_weight), project(value_weight), project(gate_weight), prior_state, lengths, decay_table(HEADS))
    half_rows = RW // N_TP
    mixed_sum = jnp.zeros((TOKENS, D), jnp.float32)
    for portion in range(N_TP):
        lower_row = portion * half_rows
        mixed_sum = mixed_sum + rounded(jnp.dot(retained[:, lower_row:lower_row + half_rows], out_weight[lower_row:lower_row + half_rows, :], preferred_element_type=jnp.float32))
    middle = rounded(tokens.astype(jnp.float32) + scaled_rows(rounded(mixed_sum), post_gain))
    moe_in = scaled_rows(middle, ffn_gain).astype(jnp.bfloat16)
    padded_in = jnp.concatenate([moe_in, jnp.zeros((1, D), jnp.bfloat16)], axis=0)
    slot_total = N_EP * CAP

    def add_expert(running, expert_id):
        matched = routes == expert_id
        chosen = jnp.any(matched, axis=1)
        weights = lax.optimization_barrier(jnp.sum(jnp.where(matched, route_gates, jnp.zeros_like(route_gates)), axis=1))
        padded_w = jnp.concatenate([weights, jnp.zeros((1,), jnp.float32)])
        picked = jnp.nonzero(chosen, size=slot_total, fill_value=TOKENS)[0].astype(jnp.int32)
        outputs = swiglu_split(padded_in[picked], expert_gate[expert_id], expert_up[expert_id], expert_down[expert_id])
        return (running.at[picked].add(padded_w[picked][:, None] * outputs.astype(jnp.float32)), None)
    routed_all = lax.scan(add_expert, jnp.zeros((TOKENS + 1, D), jnp.float32), jnp.arange(EXPERTS, dtype=jnp.int32))[0]
    shared_out = swiglu_split(moe_in, shared_gate, shared_up, shared_down)
    mixture = shared_out.astype(jnp.float32) + routed_all[:TOKENS]
    result = (middle + scaled_rows(mixture, out_gain)).astype(jnp.bfloat16)
    return (result, new_state)
```

```python
import functools

import jax
import jax.numpy as jnp
from jax import lax
from jax.experimental import pallas as pl
from jax.experimental.pallas import tpu as pltpu
from jax.sharding import PartitionSpec as P

HEAD = 64
HEADS = 16
EPS = 1e-06
THETA = 10000.0
MESH = pl.DeviceIdType.MESH
F32 = jnp.float32
BF16 = jnp.bfloat16


def rotate(vectors, lengths):
    half_dim = vectors.shape[-1] // 2
    frequency = THETA ** (-jnp.arange(half_dim, dtype=jnp.float32) / half_dim)
    angles = lengths.astype(jnp.float32)[:, None] * frequency[None, :]
    cosine = jnp.cos(angles)[:, None, :]
    sine_part = jnp.sin(angles)[:, None, :]
    leading = vectors[..., :half_dim]
    trailing = vectors[..., half_dim:]
    return jnp.concatenate(
        [leading * cosine - trailing * sine_part, trailing * cosine + leading * sine_part], axis=-1
    )


def decay_table(head_count):
    head_order = jnp.arange(head_count, dtype=jnp.float32)
    return 1.0 - jnp.exp2(-5.0 - 7.0 * head_order / (head_count - 1))


def retain(queries, keys_new, values, out_gate, prior_state, lengths, decays):
    seq_count = queries.shape[0]
    head_count = decays.shape[0]
    layout = (seq_count, head_count, HEAD)
    rot_query = rotate(queries.astype(jnp.float32).reshape(layout), lengths)
    rot_key = rotate(keys_new.astype(jnp.float32).reshape(layout), lengths) * HEAD ** (-0.5)
    wide_values = values.astype(jnp.float32).reshape(layout)
    from_state = jnp.einsum(
        "shd,shde->she", rot_query, prior_state, precision=lax.Precision.HIGHEST
    )
    self_term = jnp.sum(rot_query * rot_key, axis=-1, keepdims=True)
    read_out = decays[None, :, None] * from_state + self_term * wide_values
    new_state = (
        decays[None, :, None, None] * prior_state
        + rot_key[..., :, None] * wide_values[..., None, :]
    )
    normed = read_out * lax.rsqrt(jnp.mean(read_out * read_out, axis=-1, keepdims=True) + EPS)
    gated_rows = normed.reshape(seq_count, head_count * HEAD) * jax.nn.silu(
        out_gate.astype(jnp.float32)
    )
    return (gated_rows.astype(jnp.bfloat16), new_state)


def norm_rows(wide, gain):
    return wide * lax.rsqrt(jnp.mean(wide * wide, axis=-1, keepdims=True) + EPS) * gain


class Place:
    def __init__(self, lows, highs):
        self.lows, self.highs = lows, highs
        self.count = lows * highs
        self.ep = lax.axis_index("ep")
        self.tp = lax.axis_index("tp")
        self.hi = self.ep // lows
        self.lo = lax.rem(self.ep, lows)

    def greet(self):
        barrier = pltpu.get_barrier_semaphore()
        total = 2 * self.count
        flat = self.ep * 2 + self.tp

        def body(i, carry):
            other = lax.rem(flat + i, total)
            pl.semaphore_signal(
                barrier, inc=1, device_id=(other // 2, lax.rem(other, 2)), device_id_type=MESH
            )
            return carry

        lax.fori_loop(1, total, body, 0)
        pl.semaphore_wait(barrier, total - 1)

    def all_peers(self, source_of, target, send, recv):
        def body(i, carry):
            other = lax.rem(self.ep + i, self.count)
            start(source_of(other), target, send, recv, (other, self.tp))
            return carry

        lax.fori_loop(1, self.count, body, 0)

    def low_peers(self, source_of, target, send, recv):
        def body(i, carry):
            other = lax.rem(self.lo + i, self.lows)
            start(source_of(other), target, send, recv, (self.hi * self.lows + other, self.tp))
            return carry

        lax.fori_loop(1, self.lows, body, 0)

    def high_peers(self, source_of, target, send, recv):
        def body(i, carry):
            other = lax.rem(self.hi + i, self.highs)
            start(source_of(other), target, send, recv, (other * self.lows + self.lo, self.tp))
            return carry

        lax.fori_loop(1, self.highs, body, 0)


def start(source, target, send, recv, device):
    pltpu.make_async_remote_copy(
        src_ref=source,
        dst_ref=target,
        send_sem=send,
        recv_sem=recv,
        device_id=device,
        device_id_type=MESH,
    ).start()


def drain(span, sem):
    pltpu.make_async_copy(span, span, sem).wait()


def gather_blocks(place, own, held, sems, first):
    lows, highs = place.lows, place.highs
    place.high_peers(
        lambda other: own, held.at[place.lo, place.hi], sems.at[first], sems.at[first + 1]
    )
    arrived = held.at[0, pl.ds(0, highs - 1)]
    drain(arrived, sems.at[first + 1])
    place.low_peers(
        lambda other: held.at[place.lo], held.at[place.lo], sems.at[first + 2], sems.at[first + 3]
    )
    drain(held.at[pl.ds(0, lows - 1)], sems.at[first + 3])
    drain(arrived, sems.at[first])
    drain(held.at[pl.ds(0, lows - 1)], sems.at[first + 2])


def scatter_sums(place, part, landed, halfway, last, sems, first):
    lows, highs = place.lows, place.highs
    place.low_peers(
        lambda other: part.at[other], landed.at[place.lo], sems.at[first], sems.at[first + 1]
    )
    landed[place.lo] = part[place.lo]
    drain(landed.at[pl.ds(0, lows - 1)], sems.at[first + 1])

    def fold(h, carry):
        total = landed[0, h].astype(F32)
        for l in range(1, lows):
            total = total + landed[l, h].astype(F32)
        halfway[h] = total.astype(BF16)
        return carry

    lax.fori_loop(0, highs, fold, 0)
    place.high_peers(
        lambda other: halfway.at[other],
        last.at[place.hi],
        sems.at[first + 2],
        sems.at[first + 3],
    )
    last[place.hi] = halfway[place.hi]
    drain(last.at[pl.ds(0, highs - 1)], sems.at[first + 3])
    total = last[0].astype(F32)
    for h in range(1, highs):
        total = total + last[h].astype(F32)
    drain(part.at[pl.ds(0, lows - 1)], sems.at[first])
    drain(halfway.at[pl.ds(0, highs - 1)], sems.at[first + 2])
    return total


def project_kernel(
    lows,
    highs,
    tokens,
    gain,
    weights_q,
    weights_k,
    weights_v,
    weights_g,
    gates,
    projected,
    gates_all,
    outgoing,
    features,
    part,
    landed,
    halfway,
    last,
    sems,
):
    place = Place(lows, highs)
    count = place.count
    width = weights_q.shape[0]
    cols = weights_q.shape[1]
    normed = norm_rows(tokens[...].astype(F32), gain[...]).astype(BF16)
    for j in range(count):
        outgoing[j] = normed[:, j * width : (j + 1) * width]
    place.greet()
    place.all_peers(
        lambda other: outgoing.at[other],
        features.at[place.lo, place.hi],
        sems.at[0],
        sems.at[1],
    )
    features[place.lo, place.hi] = outgoing[place.ep]
    place.all_peers(
        lambda other: gates, gates_all.at[place.lo * highs + place.hi], sems.at[2], sems.at[3]
    )
    gates_all[place.lo * highs + place.hi] = gates[...]
    drain(outgoing.at[pl.ds(0, count - 1)], sems.at[1])
    seqs = features.shape[2]

    def multiply(l, carry):
        rows = features[l].reshape(highs * seqs, width)
        for k, weight in enumerate((weights_q, weights_k, weights_v, weights_g)):
            piece = jnp.dot(rows, weight[...], preferred_element_type=F32).astype(BF16)
            part[l, :, :, k * cols : (k + 1) * cols] = piece.reshape(highs, seqs, cols)
        return carry

    lax.fori_loop(0, lows, multiply, 0)
    total = scatter_sums(place, part, landed, halfway, last, sems, 4)
    projected[...] = total.astype(BF16)
    drain(outgoing.at[pl.ds(0, count - 1)], sems.at[0])
    drain(gates_all.at[pl.ds(0, count - 1)], sems.at[3])
    drain(gates_all.at[pl.ds(0, count - 1)], sems.at[2])


def layer_kernel(
    lows,
    highs,
    retained,
    tokens,
    out_weight,
    post_gain,
    ffn_gain,
    out_gain,
    gates_all,
    expert_gate,
    expert_up,
    expert_down,
    shared_gate,
    shared_up,
    shared_down,
    result,
    eg,
    eu,
    ed,
    sg,
    su,
    sd,
    held,
    columns,
    mixed,
    normed_all,
    part,
    landed,
    halfway,
    last,
    pair,
    local_sems,
    sems,
):
    place = Place(lows, highs)
    count = place.count
    loads = [
        pltpu.make_async_copy(source, target, local_sems.at[i])
        for i, (source, target) in enumerate(
            (
                (shared_gate, sg),
                (shared_up, su),
                (shared_down, sd),
                (expert_gate.at[0], eg),
                (expert_up.at[0], eu),
                (expert_down.at[0], ed),
            )
        )
    ]
    for load in loads:
        load.start()
    place.greet()
    seqs = tokens.shape[0]
    width = out_weight.shape[1]
    held[place.lo, place.hi] = retained[...]
    gather_blocks(place, retained, held, sems, 0)

    def multiply(l, carry):
        rows = held[l].reshape(highs * seqs, held.shape[3])
        piece = jnp.dot(rows, out_weight[...], preferred_element_type=F32).astype(BF16)
        columns[pl.ds(l * highs, highs)] = piece.reshape(highs, seqs, width)
        return carry

    lax.fori_loop(0, lows, multiply, 0)
    own_slot = place.tp * count + place.ep

    def send_back(i, carry):
        other = lax.rem(place.ep * 2 + place.tp + i, 2 * count)
        chip = other // 2
        slot = lax.rem(chip, lows) * highs + chip // lows
        start(
            columns.at[slot],
            mixed.at[own_slot],
            sems.at[4],
            sems.at[5],
            (chip, lax.rem(other, 2)),
        )
        return carry

    lax.fori_loop(1, 2 * count, send_back, 0)
    mixed[own_slot] = columns[place.lo * highs + place.hi]
    drain(mixed.at[pl.ds(0, 2 * count - 1)], sems.at[5])
    mixed_sum = jnp.concatenate(
        [(mixed[e].astype(F32) + mixed[count + e].astype(F32)) for e in range(count)], axis=1
    )
    mixed_sum = mixed_sum.astype(BF16).astype(F32)
    middle = tokens[...].astype(F32) + norm_rows(mixed_sum, post_gain[...])
    middle = middle.astype(BF16).astype(F32)
    moe_in = norm_rows(middle, ffn_gain[...]).astype(BF16)
    normed_all[place.lo, place.hi] = moe_in
    place_own = normed_all.at[place.lo, place.hi]

    gather_blocks(place, place_own, normed_all, sems, 6)
    for load in loads:
        load.wait()
    shared_hidden = (
        jax.nn.silu(jnp.dot(moe_in, sg[...], preferred_element_type=F32))
        * jnp.dot(moe_in, su[...], preferred_element_type=F32)
    ).astype(BF16)
    shared_part = jnp.dot(shared_hidden, sd[...], preferred_element_type=F32)

    chunk = max(1, min(lows, 256 // (highs * seqs)))
    chunk_rows = chunk * highs * seqs
    model = tokens.shape[1]

    def expert(i, carry):
        rows = normed_all[pl.ds(i * chunk, chunk)].reshape(chunk_rows, model)
        gate_rows = gates_all[pl.ds(i * chunk * highs, chunk * highs)].reshape(chunk_rows, count)
        lane = lax.broadcasted_iota(jnp.int32, (chunk_rows, count), 1)
        weight = jnp.sum(jnp.where(lane == place.ep, gate_rows, 0.0), axis=1, keepdims=True)
        hidden = (
            jax.nn.silu(jnp.dot(rows, eg[...], preferred_element_type=F32))
            * jnp.dot(rows, eu[...], preferred_element_type=F32)
        ).astype(BF16)
        piece = jnp.dot(hidden, ed[...], preferred_element_type=F32) * weight
        part[pl.ds(i * chunk, chunk)] = piece.astype(BF16).reshape(chunk, highs, seqs, model)
        return carry

    lax.fori_loop(0, lows // chunk, expert, 0)
    total = scatter_sums(place, part, landed, halfway, last, sems, 10)
    pair[0] = (total + shared_part).astype(BF16)
    start(pair.at[0], pair.at[1], sems.at[14], sems.at[15], (place.ep, 1 - place.tp))
    drain(pair.at[1], sems.at[15])
    mixture = pair[0].astype(F32) + pair[1].astype(F32)
    result[...] = (middle + norm_rows(mixture, out_gain[...])).astype(BF16)
    drain(mixed.at[pl.ds(0, 2 * count - 1)], sems.at[4])
    drain(pair.at[0], sems.at[14])


VM = pl.BlockSpec(memory_space=pltpu.VMEM)
FAR = pl.BlockSpec(memory_space=pl.ANY)


def on_device(
    lows,
    highs,
    tokens,
    lengths,
    prior_state,
    mix_gain,
    post_gain,
    ffn_gain,
    out_gain,
    query_weight,
    key_weight,
    value_weight,
    gate_weight,
    out_weight,
    routes,
    route_gates,
    expert_gate,
    expert_up,
    expert_down,
    shared_gate,
    shared_up,
    shared_down,
):
    count = lows * highs
    seqs, model = tokens.shape
    width, local_cols = query_weight.shape
    four = 4 * local_cols
    experts = jnp.arange(count, dtype=jnp.int32)
    gates = jnp.sum(
        jnp.where(
            routes[:, :, None] == experts[None, None, :], route_gates[:, :, None], jnp.float32(0)
        ),
        axis=1,
    )
    projected, gates_all = pl.pallas_call(
        functools.partial(project_kernel, lows, highs),
        out_shape=(
            jax.ShapeDtypeStruct((seqs, four), BF16),
            jax.ShapeDtypeStruct((count, seqs, count), F32),
        ),
        in_specs=[VM] * 7,
        out_specs=(VM, VM),
        scratch_shapes=[
            pltpu.VMEM((count, seqs, width), BF16),
            pltpu.VMEM((lows, highs, seqs, width), BF16),
            pltpu.VMEM((lows, highs, seqs, four), BF16),
            pltpu.VMEM((lows, highs, seqs, four), BF16),
            pltpu.VMEM((highs, seqs, four), BF16),
            pltpu.VMEM((highs, seqs, four), BF16),
            pltpu.SemaphoreType.DMA((8,)),
        ],
        compiler_params=pltpu.CompilerParams(collective_id=0, has_side_effects=True),
        name="project",
    )(
        tokens,
        mix_gain.reshape(1, -1),
        query_weight,
        key_weight,
        value_weight,
        gate_weight,
        gates,
    )
    queries, keys_new, values, out_gate = tuple(
        projected[:, role * local_cols : (role + 1) * local_cols] for role in range(4)
    )
    heads_here = local_cols // HEAD
    decays = lax.dynamic_slice_in_dim(
        decay_table(HEADS), lax.axis_index("tp") * heads_here, heads_here, 0
    )
    retained, new_state = retain(queries, keys_new, values, out_gate, prior_state, lengths, decays)
    hidden_cols = expert_gate.shape[2]
    shared_cols = shared_gate.shape[1]
    result = pl.pallas_call(
        functools.partial(layer_kernel, lows, highs),
        out_shape=jax.ShapeDtypeStruct((seqs, model), BF16),
        in_specs=[VM] * 7 + [FAR] * 6,
        out_specs=VM,
        scratch_shapes=[
            pltpu.VMEM((model, hidden_cols), BF16),
            pltpu.VMEM((model, hidden_cols), BF16),
            pltpu.VMEM((hidden_cols, model), BF16),
            pltpu.VMEM((model, shared_cols), BF16),
            pltpu.VMEM((model, shared_cols), BF16),
            pltpu.VMEM((shared_cols, model), BF16),
            pltpu.VMEM((lows, highs, seqs, local_cols), BF16),
            pltpu.VMEM((count, seqs, width), BF16),
            pltpu.VMEM((2 * count, seqs, width), BF16),
            pltpu.VMEM((lows, highs, seqs, model), BF16),
            pltpu.VMEM((lows, highs, seqs, model), BF16),
            pltpu.VMEM((lows, highs, seqs, model), BF16),
            pltpu.VMEM((highs, seqs, model), BF16),
            pltpu.VMEM((highs, seqs, model), BF16),
            pltpu.VMEM((2, seqs, model), BF16),
            pltpu.SemaphoreType.DMA((6,)),
            pltpu.SemaphoreType.DMA((16,)),
        ],
        compiler_params=pltpu.CompilerParams(collective_id=1, has_side_effects=True),
        name="layer",
    )(
        retained,
        tokens,
        out_weight,
        post_gain.reshape(1, -1),
        ffn_gain.reshape(1, -1),
        out_gain.reshape(1, -1),
        gates_all,
        expert_gate,
        expert_up,
        expert_down,
        shared_gate,
        shared_up,
        shared_down,
    )
    return (result, new_state)


def solution(mesh):
    count = mesh.shape["ep"]
    lows = 1
    while lows * lows < count:
        lows *= 2
    highs = count // lows
    return jax.shard_map(
        functools.partial(on_device, lows, highs),
        mesh=mesh,
        in_specs=(
            P("ep", None),
            P("ep"),
            P("ep", "tp", None, None),
            P(),
            P(),
            P(),
            P(),
            P("ep", "tp"),
            P("ep", "tp"),
            P("ep", "tp"),
            P("ep", "tp"),
            P("tp", "ep"),
            P("ep", None),
            P("ep", None),
            P("ep", None, "tp"),
            P("ep", None, "tp"),
            P("ep", "tp", None),
            P(None, "tp"),
            P(None, "tp"),
            P("tp", None),
        ),
        out_specs=(P("ep", None), P("ep", "tp", None, None)),
        check_vma=False,
    )
```

```python
import functools

import jax
import jax.numpy as jnp
from jax import lax
from jax.experimental import pallas as pl
from jax.experimental.pallas import tpu as pltpu
from jax.sharding import PartitionSpec as P

HEAD = 64
HEADS = 16
EPS = 1e-06
THETA = 10000.0
MESH = pl.DeviceIdType.MESH
F32 = jnp.float32
BF16 = jnp.bfloat16


def rotate(vectors, lengths):
    half_dim = vectors.shape[-1] // 2
    frequency = THETA ** (-jnp.arange(half_dim, dtype=jnp.float32) / half_dim)
    angles = lengths.astype(jnp.float32)[:, None] * frequency[None, :]
    cosine = jnp.cos(angles)[:, None, :]
    sine_part = jnp.sin(angles)[:, None, :]
    leading = vectors[..., :half_dim]
    trailing = vectors[..., half_dim:]
    return jnp.concatenate(
        [leading * cosine - trailing * sine_part, trailing * cosine + leading * sine_part], axis=-1
    )


def decay_table(head_count):
    head_order = jnp.arange(head_count, dtype=jnp.float32)
    return 1.0 - jnp.exp2(-5.0 - 7.0 * head_order / (head_count - 1))


def retain(queries, keys_new, values, out_gate, prior_state, lengths, decays):
    seq_count = queries.shape[0]
    head_count = decays.shape[0]
    layout = (seq_count, head_count, HEAD)
    rot_query = rotate(queries.astype(jnp.float32).reshape(layout), lengths)
    rot_key = rotate(keys_new.astype(jnp.float32).reshape(layout), lengths) * HEAD ** (-0.5)
    wide_values = values.astype(jnp.float32).reshape(layout)
    from_state = jnp.einsum(
        "shd,shde->she", rot_query, prior_state, precision=lax.Precision.HIGHEST
    )
    self_term = jnp.sum(rot_query * rot_key, axis=-1, keepdims=True)
    read_out = decays[None, :, None] * from_state + self_term * wide_values
    new_state = (
        decays[None, :, None, None] * prior_state
        + rot_key[..., :, None] * wide_values[..., None, :]
    )
    normed = read_out * lax.rsqrt(jnp.mean(read_out * read_out, axis=-1, keepdims=True) + EPS)
    gated_rows = normed.reshape(seq_count, head_count * HEAD) * jax.nn.silu(
        out_gate.astype(jnp.float32)
    )
    return (gated_rows.astype(jnp.bfloat16), new_state)


def norm_rows(wide, gain):
    return wide * lax.rsqrt(jnp.mean(wide * wide, axis=-1, keepdims=True) + EPS) * gain


class Place:
    def __init__(self, lows, highs):
        self.lows, self.highs = lows, highs
        self.count = lows * highs
        self.ep = lax.axis_index("ep")
        self.tp = lax.axis_index("tp")
        self.hi = self.ep // lows
        self.lo = lax.rem(self.ep, lows)

    def greet(self):
        barrier = pltpu.get_barrier_semaphore()
        total = 2 * self.count
        flat = self.ep * 2 + self.tp

        def body(i, carry):
            other = lax.rem(flat + i, total)
            pl.semaphore_signal(
                barrier, inc=1, device_id=(other // 2, lax.rem(other, 2)), device_id_type=MESH
            )
            return carry

        lax.fori_loop(1, total, body, 0)
        pl.semaphore_wait(barrier, total - 1)

    def all_peers(self, source_of, target, send, recv):
        def body(i, carry):
            other = lax.rem(self.ep + i, self.count)
            start(source_of(other), target, send, recv, (other, self.tp))
            return carry

        lax.fori_loop(1, self.count, body, 0)

    def low_peers(self, source_of, target, send, recv):
        def body(i, carry):
            other = lax.rem(self.lo + i, self.lows)
            start(source_of(other), target, send, recv, (self.hi * self.lows + other, self.tp))
            return carry

        lax.fori_loop(1, self.lows, body, 0)

    def high_peers(self, source_of, target, send, recv):
        def body(i, carry):
            other = lax.rem(self.hi + i, self.highs)
            start(source_of(other), target, send, recv, (other * self.lows + self.lo, self.tp))
            return carry

        lax.fori_loop(1, self.highs, body, 0)


def start(source, target, send, recv, device):
    pltpu.make_async_remote_copy(
        src_ref=source,
        dst_ref=target,
        send_sem=send,
        recv_sem=recv,
        device_id=device,
        device_id_type=MESH,
    ).start()


def drain(span, sem):
    pltpu.make_async_copy(span, span, sem).wait()


def gather_blocks(place, held, send, near, far, during=None, arrived=None):
    lows, highs = place.lows, place.highs
    own = held.at[place.lo, place.hi]
    place.high_peers(lambda other: own, own, send.at[0], far.at[place.hi])
    place.low_peers(lambda other: own, own, send.at[1], near.at[place.hi])
    if during is not None:
        during()
    for i in range(1, highs):
        h = lax.rem(place.hi + highs - i, highs)
        block = held.at[place.lo, h]
        drain(block, far.at[h])
        place.low_peers(lambda other: block, block, send.at[1], near.at[h])
    for i in range(highs):
        h = lax.rem(place.hi + highs - i, highs)
        drain(held.at[pl.ds(0, lows - 1), h], near.at[h])
        if arrived is not None:
            arrived(h)

    def finish():
        drain(held.at[0, pl.ds(0, highs - 1)], send.at[0])
        drain(held.at[pl.ds(0, lows - 1)], send.at[1])

    return finish


def scatter_sums(place, fill, part, landed, halfway, last, send, near, far):
    lows, highs = place.lows, place.highs
    chunks = part.shape[0]
    for c in range(chunks):
        fill(c)
        place.low_peers(
            lambda other: part.at[c, other], landed.at[c, place.lo], send.at[0], near.at[c]
        )
        landed[c, place.lo] = part[c, place.lo]
    for c in range(chunks):
        drain(landed.at[c, pl.ds(0, lows - 1)], near.at[c])

        def fold(h, carry):
            total = landed[c, 0, h].astype(F32)
            for l in range(1, lows):
                total = total + landed[c, l, h].astype(F32)
            halfway[c, h] = total.astype(BF16)
            return carry

        lax.fori_loop(0, highs, fold, 0)
        place.high_peers(
            lambda other: halfway.at[c, other], last.at[c, place.hi], send.at[1], far.at[c]
        )
        last[c, place.hi] = halfway[c, place.hi]
    sums = []
    for c in range(chunks):
        drain(last.at[c, pl.ds(0, highs - 1)], far.at[c])
        total = last[c, 0].astype(F32)
        for h in range(1, highs):
            total = total + last[c, h].astype(F32)
        sums.append(total)

    def finish():
        drain(part.at[:, pl.ds(0, lows - 1)], send.at[0])
        drain(halfway.at[:, pl.ds(0, highs - 1)], send.at[1])

    return sums, finish


def project_kernel(
    lows,
    highs,
    tokens,
    gain,
    weights_q,
    weights_k,
    weights_v,
    weights_g,
    gates,
    projected,
    gates_all,
    outgoing,
    features,
    part,
    landed,
    halfway,
    last,
    sems,
    send,
    near,
    far,
):
    place = Place(lows, highs)
    count = place.count
    width = weights_q.shape[0]
    cols = weights_q.shape[1]
    normed = norm_rows(tokens[...].astype(F32), gain[...]).astype(BF16)
    for j in range(count):
        outgoing[j] = normed[:, j * width : (j + 1) * width]
    place.greet()
    place.all_peers(
        lambda other: outgoing.at[other],
        features.at[place.lo, place.hi],
        sems.at[0],
        sems.at[1],
    )
    features[place.lo, place.hi] = outgoing[place.ep]
    place.all_peers(
        lambda other: gates, gates_all.at[place.lo * highs + place.hi], sems.at[2], sems.at[3]
    )
    gates_all[place.lo * highs + place.hi] = gates[...]
    drain(outgoing.at[pl.ds(0, count - 1)], sems.at[1])
    seqs = features.shape[2]
    weights = (weights_q, weights_k, weights_v, weights_g)

    def fill(c):
        def multiply(l, carry):
            rows = features[l].reshape(highs * seqs, width)
            piece = jnp.dot(rows, weights[c][...], preferred_element_type=F32).astype(BF16)
            part[c, l] = piece.reshape(highs, seqs, cols)
            return carry

        lax.fori_loop(0, lows, multiply, 0)

    sums, finish = scatter_sums(place, fill, part, landed, halfway, last, send, near, far)
    for c in range(4):
        projected[:, c * cols : (c + 1) * cols] = sums[c].astype(BF16)
    finish()
    drain(outgoing.at[pl.ds(0, count - 1)], sems.at[0])
    drain(gates_all.at[pl.ds(0, count - 1)], sems.at[3])
    drain(gates_all.at[pl.ds(0, count - 1)], sems.at[2])


def layer_kernel(
    lows,
    highs,
    retained,
    tokens,
    out_weight,
    post_gain,
    ffn_gain,
    out_gain,
    gates_all,
    expert_gate,
    expert_up,
    expert_down,
    shared_gate,
    shared_up,
    shared_down,
    result,
    eg,
    eu,
    ed,
    sg,
    su,
    sd,
    held,
    columns,
    mixed,
    normed_all,
    gate_sum,
    up_sum,
    hidden,
    shared_pair,
    give,
    theirs,
    part,
    landed,
    halfway,
    last,
    pair,
    local_sems,
    sems,
    held_send,
    held_near,
    held_far,
    all_send,
    all_near,
    all_far,
    all_twin,
    sum_send,
    sum_near,
    sum_far,
    sum_twin,
):
    place = Place(lows, highs)
    count = place.count
    twin = (place.ep, 1 - place.tp)
    loads = [
        pltpu.make_async_copy(source, target, local_sems.at[i])
        for i, (source, target) in enumerate(
            (
                (shared_gate, sg),
                (shared_up, su),
                (shared_down, sd),
                (expert_gate.at[0], eg),
                (expert_up.at[0], eu),
                (expert_down.at[0], ed),
            )
        )
    ]
    for load in loads:
        load.start()
    place.greet()
    seqs, model = tokens.shape
    half = model // 2
    width = out_weight.shape[1]
    held[place.lo, place.hi] = retained[...]
    finish_held = gather_blocks(place, held, held_send, held_near, held_far)

    def multiply(l, carry):
        rows = held[l].reshape(highs * seqs, held.shape[3])
        piece = jnp.dot(rows, out_weight[...], preferred_element_type=F32).astype(BF16)
        columns[pl.ds(l * highs, highs)] = piece.reshape(highs, seqs, width)
        return carry

    lax.fori_loop(0, lows, multiply, 0)
    own_slot = place.tp * count + place.ep

    def send_back(i, carry):
        other = lax.rem(place.ep * 2 + place.tp + i, 2 * count)
        chip = other // 2
        slot = lax.rem(chip, lows) * highs + chip // lows
        start(
            columns.at[slot],
            mixed.at[own_slot],
            sems.at[0],
            sems.at[1],
            (chip, lax.rem(other, 2)),
        )
        return carry

    lax.fori_loop(1, 2 * count, send_back, 0)
    mixed[own_slot] = columns[place.lo * highs + place.hi]
    for load in loads:
        load.wait()
    drain(mixed.at[pl.ds(0, 2 * count - 1)], sems.at[1])
    mixed_sum = jnp.concatenate(
        [(mixed[e].astype(F32) + mixed[count + e].astype(F32)) for e in range(count)], axis=1
    )
    mixed_sum = mixed_sum.astype(BF16).astype(F32)
    middle = tokens[...].astype(F32) + norm_rows(mixed_sum, post_gain[...])
    middle = middle.astype(BF16).astype(F32)
    moe_in = norm_rows(middle, ffn_gain[...]).astype(BF16)
    own_half = jnp.where(place.tp == 0, moe_in[:, :half], moe_in[:, half:])
    normed_all[place.tp, place.lo, place.hi] = own_half
    mine = normed_all.at[place.tp]

    def shared():
        shared_hidden = (
            jax.nn.silu(jnp.dot(moe_in, sg[...], preferred_element_type=F32))
            * jnp.dot(moe_in, su[...], preferred_element_type=F32)
        ).astype(BF16)
        shared_part = jnp.dot(shared_hidden, sd[...], preferred_element_type=F32).astype(BF16)
        for t in range(2):
            shared_pair[t] = shared_part[:, t * half : (t + 1) * half]
        start(shared_pair.at[1 - place.tp], shared_pair.at[2], sems.at[2], sems.at[3], twin)

    def hand_over(h):
        start(
            mine.at[:, h],
            normed_all.at[place.tp, :, h],
            sems.at[4],
            all_twin,
            twin,
        )

    finish_all = gather_blocks(place, mine, all_send, all_near, all_far, shared, hand_over)

    chunk = max(1, min(lows, 256 // (highs * seqs)))
    chunk_rows = chunk * highs * seqs
    steps = lows // chunk
    own_rows = pl.ds(pl.multiple_of(place.tp * half, half), half)
    other_rows = pl.ds(pl.multiple_of((1 - place.tp) * half, half), half)

    def near_half(i, carry):
        rows = normed_all[place.tp, pl.ds(i * chunk, chunk)].reshape(chunk_rows, half)
        gate_sum[i] = jnp.dot(rows, eg[own_rows, :], preferred_element_type=F32)
        up_sum[i] = jnp.dot(rows, eu[own_rows, :], preferred_element_type=F32)
        return carry

    lax.fori_loop(0, steps, near_half, 0)
    drain(normed_all.at[1 - place.tp], all_twin)

    def far_half(i, carry):
        rows = normed_all[1 - place.tp, pl.ds(i * chunk, chunk)].reshape(chunk_rows, half)
        gate_cols = gate_sum[i] + jnp.dot(rows, eg[other_rows, :], preferred_element_type=F32)
        up_cols = up_sum[i] + jnp.dot(rows, eu[other_rows, :], preferred_element_type=F32)
        hidden[i] = (jax.nn.silu(gate_cols) * up_cols).astype(BF16)
        return carry

    lax.fori_loop(0, steps, far_half, 0)
    cols = part.shape[4]

    def down(i, first):
        gate_rows = gates_all[pl.ds(i * chunk * highs, chunk * highs)].reshape(chunk_rows, count)
        lane = lax.broadcasted_iota(jnp.int32, (chunk_rows, count), 1)
        weight = jnp.sum(jnp.where(lane == place.ep, gate_rows, 0.0), axis=1, keepdims=True)
        span = pl.ds(pl.multiple_of(first, cols), cols)
        return jnp.dot(hidden[i], ed[:, span], preferred_element_type=F32) * weight

    for c in range(part.shape[0]):

        def outward(i, carry):
            piece = down(i, (1 - place.tp) * half + c * cols).astype(BF16)
            give[c, pl.ds(i * chunk, chunk)] = piece.reshape(chunk, highs, seqs, cols)
            return carry

        lax.fori_loop(0, steps, outward, 0)
        start(give.at[c], theirs.at[c], sems.at[5], sum_twin.at[c], twin)

    def fill(c):
        drain(theirs.at[c], sum_twin.at[c])

        def inward(i, carry):
            piece = down(i, place.tp * half + c * cols)
            other = theirs[c, pl.ds(i * chunk, chunk)].reshape(chunk_rows, cols).astype(F32)
            piece = (piece + other).astype(BF16)
            part[c, pl.ds(i * chunk, chunk)] = piece.reshape(chunk, highs, seqs, cols)
            return carry

        lax.fori_loop(0, steps, inward, 0)

    sums, finish_sums = scatter_sums(
        place, fill, part, landed, halfway, last, sum_send, sum_near, sum_far
    )
    drain(shared_pair.at[2], sems.at[3])
    pair[place.tp] = jnp.concatenate(sums, axis=1) + (
        shared_pair[place.tp].astype(F32) + shared_pair[2].astype(F32)
    )
    start(pair.at[place.tp], pair.at[place.tp], sems.at[6], sems.at[7], twin)
    drain(pair.at[1 - place.tp], sems.at[7])
    mixture = jnp.concatenate([pair[0], pair[1]], axis=1)
    result[...] = (middle + norm_rows(mixture, out_gain[...])).astype(BF16)
    finish_held()
    finish_all()
    finish_sums()
    drain(mixed.at[pl.ds(0, 2 * count - 1)], sems.at[0])
    drain(shared_pair.at[2], sems.at[2])
    drain(mine, sems.at[4])
    drain(give, sems.at[5])
    drain(pair.at[0], sems.at[6])


VM = pl.BlockSpec(memory_space=pltpu.VMEM)
FAR = pl.BlockSpec(memory_space=pl.ANY)


def on_device(
    lows,
    highs,
    tokens,
    lengths,
    prior_state,
    mix_gain,
    post_gain,
    ffn_gain,
    out_gain,
    query_weight,
    key_weight,
    value_weight,
    gate_weight,
    out_weight,
    routes,
    route_gates,
    expert_gate,
    expert_up,
    expert_down,
    shared_gate,
    shared_up,
    shared_down,
):
    count = lows * highs
    seqs, model = tokens.shape
    width, local_cols = query_weight.shape
    four = 4 * local_cols
    experts = jnp.arange(count, dtype=jnp.int32)
    gates = jnp.sum(
        jnp.where(
            routes[:, :, None] == experts[None, None, :], route_gates[:, :, None], jnp.float32(0)
        ),
        axis=1,
    )
    projected, gates_all = pl.pallas_call(
        functools.partial(project_kernel, lows, highs),
        out_shape=(
            jax.ShapeDtypeStruct((seqs, four), BF16),
            jax.ShapeDtypeStruct((count, seqs, count), F32),
        ),
        in_specs=[VM] * 7,
        out_specs=(VM, VM),
        scratch_shapes=[
            pltpu.VMEM((count, seqs, width), BF16),
            pltpu.VMEM((lows, highs, seqs, width), BF16),
            pltpu.VMEM((4, lows, highs, seqs, local_cols), BF16),
            pltpu.VMEM((4, lows, highs, seqs, local_cols), BF16),
            pltpu.VMEM((4, highs, seqs, local_cols), BF16),
            pltpu.VMEM((4, highs, seqs, local_cols), BF16),
            pltpu.SemaphoreType.DMA((4,)),
            pltpu.SemaphoreType.DMA((2,)),
            pltpu.SemaphoreType.DMA((4,)),
            pltpu.SemaphoreType.DMA((4,)),
        ],
        compiler_params=pltpu.CompilerParams(collective_id=0, has_side_effects=True),
        name="project",
    )(
        tokens,
        mix_gain.reshape(1, -1),
        query_weight,
        key_weight,
        value_weight,
        gate_weight,
        gates,
    )
    queries, keys_new, values, out_gate = tuple(
        projected[:, role * local_cols : (role + 1) * local_cols] for role in range(4)
    )
    heads_here = local_cols // HEAD
    decays = lax.dynamic_slice_in_dim(
        decay_table(HEADS), lax.axis_index("tp") * heads_here, heads_here, 0
    )
    retained, new_state = retain(queries, keys_new, values, out_gate, prior_state, lengths, decays)
    hidden_cols = expert_gate.shape[2]
    shared_cols = shared_gate.shape[1]
    half = model // 2
    chunks = 4
    steps = lows // max(1, min(lows, 256 // (highs * seqs)))
    result = pl.pallas_call(
        functools.partial(layer_kernel, lows, highs),
        out_shape=jax.ShapeDtypeStruct((seqs, model), BF16),
        in_specs=[VM] * 7 + [FAR] * 6,
        out_specs=VM,
        scratch_shapes=[
            pltpu.VMEM((model, hidden_cols), BF16),
            pltpu.VMEM((model, hidden_cols), BF16),
            pltpu.VMEM((hidden_cols, model), BF16),
            pltpu.VMEM((model, shared_cols), BF16),
            pltpu.VMEM((model, shared_cols), BF16),
            pltpu.VMEM((shared_cols, model), BF16),
            pltpu.VMEM((lows, highs, seqs, local_cols), BF16),
            pltpu.VMEM((count, seqs, width), BF16),
            pltpu.VMEM((2 * count, seqs, width), BF16),
            pltpu.VMEM((2, lows, highs, seqs, half), BF16),
            pltpu.VMEM((steps, count * seqs // steps, hidden_cols), F32),
            pltpu.VMEM((steps, count * seqs // steps, hidden_cols), F32),
            pltpu.VMEM((steps, count * seqs // steps, hidden_cols), BF16),
            pltpu.VMEM((3, seqs, half), BF16),
            pltpu.VMEM((chunks, lows, highs, seqs, half // chunks), BF16),
            pltpu.VMEM((chunks, lows, highs, seqs, half // chunks), BF16),
            pltpu.VMEM((chunks, lows, highs, seqs, half // chunks), BF16),
            pltpu.VMEM((chunks, lows, highs, seqs, half // chunks), BF16),
            pltpu.VMEM((chunks, highs, seqs, half // chunks), BF16),
            pltpu.VMEM((chunks, highs, seqs, half // chunks), BF16),
            pltpu.VMEM((2, seqs, half), F32),
            pltpu.SemaphoreType.DMA((6,)),
            pltpu.SemaphoreType.DMA((8,)),
            pltpu.SemaphoreType.DMA((2,)),
            pltpu.SemaphoreType.DMA((highs,)),
            pltpu.SemaphoreType.DMA((highs,)),
            pltpu.SemaphoreType.DMA((2,)),
            pltpu.SemaphoreType.DMA((highs,)),
            pltpu.SemaphoreType.DMA((highs,)),
            pltpu.SemaphoreType.DMA,
            pltpu.SemaphoreType.DMA((2,)),
            pltpu.SemaphoreType.DMA((chunks,)),
            pltpu.SemaphoreType.DMA((chunks,)),
            pltpu.SemaphoreType.DMA((chunks,)),
        ],
        compiler_params=pltpu.CompilerParams(collective_id=1, has_side_effects=True),
        name="layer",
    )(
        retained,
        tokens,
        out_weight,
        post_gain.reshape(1, -1),
        ffn_gain.reshape(1, -1),
        out_gain.reshape(1, -1),
        gates_all,
        expert_gate,
        expert_up,
        expert_down,
        shared_gate,
        shared_up,
        shared_down,
    )
    return (result, new_state)


def solution(mesh):
    count = mesh.shape["ep"]
    lows = 1
    while lows * lows < count:
        lows *= 2
    highs = count // lows
    return jax.shard_map(
        functools.partial(on_device, lows, highs),
        mesh=mesh,
        in_specs=(
            P("ep", None),
            P("ep"),
            P("ep", "tp", None, None),
            P(),
            P(),
            P(),
            P(),
            P("ep", "tp"),
            P("ep", "tp"),
            P("ep", "tp"),
            P("ep", "tp"),
            P("tp", "ep"),
            P("ep", None),
            P("ep", None),
            P("ep", None, "tp"),
            P("ep", None, "tp"),
            P("ep", "tp", None),
            P(None, "tp"),
            P(None, "tp"),
            P("tp", None),
        ),
        out_specs=(P("ep", None), P("ep", "tp", None, None)),
        check_vma=False,
    )
```

```python
import functools

import jax
import jax.numpy as jnp
from jax import lax
from jax.experimental import pallas as pl
from jax.experimental.pallas import tpu as pltpu
from jax.sharding import PartitionSpec as P

HEAD = 64
HEADS = 16
EPS = 1e-06
THETA = 10000.0
MESH = pl.DeviceIdType.MESH
F32 = jnp.float32
BF16 = jnp.bfloat16


def decay_table(head_count):
    head_order = jnp.arange(head_count, dtype=jnp.float32)
    return 1.0 - jnp.exp2(-5.0 - 7.0 * head_order / (head_count - 1))


def norm_rows(wide, gain):
    return wide * lax.rsqrt(jnp.mean(wide * wide, axis=-1, keepdims=True) + EPS) * gain


class Place:
    def __init__(self, lows, highs):
        self.lows, self.highs = lows, highs
        self.count = lows * highs
        self.ep = lax.axis_index("ep")
        self.tp = lax.axis_index("tp")
        self.hi = self.ep // lows
        self.lo = lax.rem(self.ep, lows)

    def greet(self):
        barrier = pltpu.get_barrier_semaphore()
        total = 2 * self.count
        flat = self.ep * 2 + self.tp

        def body(i, carry):
            other = lax.rem(flat + i, total)
            pl.semaphore_signal(
                barrier, inc=1, device_id=(other // 2, lax.rem(other, 2)), device_id_type=MESH
            )
            return carry

        lax.fori_loop(1, total, body, 0)
        return lambda: pl.semaphore_wait(barrier, total - 1)

    def all_peers(self, source_of, target, send, recv):
        def body(i, carry):
            other = lax.rem(self.ep + i, self.count)
            start(source_of(other), target, send, recv, (other, self.tp))
            return carry

        lax.fori_loop(1, self.count, body, 0)

    def low_peers(self, source_of, target, send, recv):
        def body(i, carry):
            other = lax.rem(self.lo + i, self.lows)
            start(source_of(other), target, send, recv, (self.hi * self.lows + other, self.tp))
            return carry

        lax.fori_loop(1, self.lows, body, 0)

    def high_peers(self, source_of, target, send, recv):
        def body(i, carry):
            other = lax.rem(self.hi + i, self.highs)
            start(source_of(other), target, send, recv, (other * self.lows + self.lo, self.tp))
            return carry

        lax.fori_loop(1, self.highs, body, 0)


def start(source, target, send, recv, device):
    pltpu.make_async_remote_copy(
        src_ref=source,
        dst_ref=target,
        send_sem=send,
        recv_sem=recv,
        device_id=device,
        device_id_type=MESH,
    ).start()


def drain(span, sem):
    pltpu.make_async_copy(span, span, sem).wait()


def gather_blocks(place, held, send, near, far, during=None, arrived=None):
    lows, highs = place.lows, place.highs
    own = held.at[place.lo, place.hi]
    place.high_peers(lambda other: own, own, send.at[0], far.at[place.hi])
    place.low_peers(lambda other: own, own, send.at[1], near.at[place.hi])
    if during is not None:
        during()
    for i in range(1, highs):
        h = lax.rem(place.hi + highs - i, highs)
        block = held.at[place.lo, h]
        drain(block, far.at[h])
        place.low_peers(lambda other: block, block, send.at[1], near.at[h])
    for i in range(highs):
        h = lax.rem(place.hi + highs - i, highs)
        drain(held.at[pl.ds(0, lows - 1), h], near.at[h])
        if arrived is not None:
            arrived(h)

    def finish():
        drain(held.at[0, pl.ds(0, highs - 1)], send.at[0])
        drain(held.at[pl.ds(0, lows - 1)], send.at[1])

    return finish


def scatter_sums(place, fill, part, landed, halfway, last, send, near, far):
    lows, highs = place.lows, place.highs
    chunks = part.shape[0]
    for c in range(chunks):
        fill(c)
        place.low_peers(
            lambda other: part.at[c, other], landed.at[c, place.lo], send.at[0], near.at[c]
        )
        landed[c, place.lo] = part[c, place.lo]
    for c in range(chunks):
        drain(landed.at[c, pl.ds(0, lows - 1)], near.at[c])

        def fold(h, carry):
            total = landed[c, 0, h].astype(F32)
            for l in range(1, lows):
                total = total + landed[c, l, h].astype(F32)
            halfway[c, h] = total.astype(BF16)
            return carry

        lax.fori_loop(0, highs, fold, 0)
        place.high_peers(
            lambda other: halfway.at[c, other], last.at[c, place.hi], send.at[1], far.at[c]
        )
        last[c, place.hi] = halfway[c, place.hi]
    sums = []
    for c in range(chunks):
        drain(last.at[c, pl.ds(0, highs - 1)], far.at[c])
        total = last[c, 0].astype(F32)
        for h in range(1, highs):
            total = total + last[c, h].astype(F32)
        sums.append(total)

    def finish():
        drain(part.at[:, pl.ds(0, lows - 1)], send.at[0])
        drain(halfway.at[:, pl.ds(0, highs - 1)], send.at[1])

    return sums, finish


def project(
    place,
    enter,
    tokens,
    gain,
    routes,
    route_gates,
    weights,
    weight_loads,
    gates_all,
    outgoing,
    features,
    part,
    landed,
    halfway,
    last,
    sems,
    send,
    near,
    far,
):
    lows, highs, count = place.lows, place.highs, place.count
    _, width, cols = weights.shape
    seqs = tokens.shape[0]
    normed = norm_rows(tokens[...].astype(F32), gain[...]).astype(BF16)
    for j in range(count):
        outgoing[j] = normed[:, j * width : (j + 1) * width]
    features[place.lo, place.hi] = outgoing[place.ep]
    lane = lax.broadcasted_iota(jnp.int32, (seqs, count), 1)
    dense = jnp.zeros((seqs, count), F32)
    for k in range(routes.shape[1]):
        dense = dense + jnp.where(lane == routes[:, k : k + 1], route_gates[:, k : k + 1], 0.0)
    own = place.lo * highs + place.hi
    gates_all[own] = dense
    enter()
    place.all_peers(
        lambda other: outgoing.at[other],
        features.at[place.lo, place.hi],
        sems.at[0],
        sems.at[1],
    )
    for load in weight_loads:
        load.wait()
    drain(outgoing.at[pl.ds(0, count - 1)], sems.at[1])

    def fill(c):
        def multiply(l, carry):
            rows = features[l].reshape(highs * seqs, width)
            piece = jnp.dot(rows, weights[c], preferred_element_type=F32).astype(BF16)
            part[c, l] = piece.reshape(highs, seqs, cols)
            return carry

        lax.fori_loop(0, lows, multiply, 0)

    sums, finish = scatter_sums(place, fill, part, landed, halfway, last, send, near, far)
    place.all_peers(lambda other: gates_all.at[own], gates_all.at[own], sems.at[2], sems.at[3])

    def finish_all():
        finish()
        drain(outgoing.at[pl.ds(0, count - 1)], sems.at[0])
        drain(gates_all.at[pl.ds(0, count - 1)], sems.at[2])

    return [total.astype(BF16) for total in sums], finish_all


def head_sums(values):
    rows, cols = values.shape
    pair = 2 * HEAD
    row_of = lax.broadcasted_iota(jnp.int32, (pair, pair), 0) // HEAD
    col_of = lax.broadcasted_iota(jnp.int32, (pair, pair), 1) // HEAD
    ones = jnp.where(row_of == col_of, 1.0, 0.0).astype(F32)
    groups = cols // pair
    stacked = jnp.concatenate([values[:, g * pair : (g + 1) * pair] for g in range(groups)], axis=0)
    summed = jnp.dot(
        stacked, ones, preferred_element_type=F32, precision=lax.Precision.HIGHEST
    )
    return jnp.concatenate([summed[g * rows : (g + 1) * rows] for g in range(groups)], axis=1)


def retain(place, projected, cosine, sine, state, turned, read):
    queries, keys_new, values, out_gate = [member.astype(F32) for member in projected]
    seqs, cols = queries.shape
    lane = lax.broadcasted_iota(jnp.int32, (seqs, cols), 1)
    leading = lax.rem(lane, HEAD) < HEAD // 2

    def rotate(x):
        swapped = jnp.where(
            leading, pltpu.roll(x, cols - HEAD // 2, axis=1), pltpu.roll(x, HEAD // 2, axis=1)
        )
        return x * cosine[...] + swapped * sine[...]

    rot_query = rotate(queries)
    rot_key = rotate(keys_new) * HEAD ** (-0.5)
    turned[...] = rot_query
    pair = 2 * HEAD
    deep = lax.broadcasted_iota(jnp.int32, (HEAD, pair), 0)
    wide = lax.broadcasted_iota(jnp.int32, (HEAD, pair), 1)
    picks = [wide == deep, wide == deep + HEAD]

    def one_row(s, carry):
        row = turned[pl.ds(s, 1), :]
        for h in range(cols // HEAD):
            both = row[:, (h // 2) * pair : (h // 2 + 1) * pair]
            column = jnp.sum(
                jnp.where(picks[h % 2], jnp.broadcast_to(both, (HEAD, pair)), 0.0),
                axis=1,
                keepdims=True,
            )
            read[h, pl.ds(s, 1), :] = jnp.sum(column * state[s, h], axis=0, keepdims=True)
        return carry

    lax.fori_loop(0, seqs, one_row, 0)
    from_state = jnp.concatenate([read[h] for h in range(cols // HEAD)], axis=1)
    head = (place.tp * (cols // HEAD) + lane // HEAD).astype(F32)
    decays = 1.0 - jnp.exp2(-5.0 - 7.0 * head / (HEADS - 1))
    read_out = decays * from_state + head_sums(rot_query * rot_key) * values
    normed = read_out * lax.rsqrt(head_sums(read_out * read_out) / HEAD + EPS)
    return (normed * jax.nn.silu(out_gate)).astype(BF16), rot_key


def layer_kernel(
    lows,
    highs,
    tokens,
    cosine,
    sine,
    routes,
    route_gates,
    mix_gain,
    post_gain,
    ffn_gain,
    out_gain,
    prior_state,
    query_weight,
    key_weight,
    value_weight,
    gate_weight,
    out_weight_far,
    expert_gate,
    expert_up,
    expert_down,
    shared_gate,
    shared_up,
    shared_down,
    result,
    key_out,
    value_out,
    weights,
    out_weight,
    state,
    eg,
    eu,
    ed,
    sg,
    su,
    sd,
    gates_all,
    outgoing,
    features,
    first_part,
    first_landed,
    first_halfway,
    first_last,
    turned,
    read,
    held,
    columns,
    mixed,
    normed_all,
    gate_sum,
    up_sum,
    hidden,
    shared_pair,
    give,
    part,
    landed,
    halfway,
    last,
    pair,
    local_sems,
    sems,
    first_sems,
    first_send,
    first_near,
    first_far,
    held_send,
    held_near,
    held_far,
    all_send,
    all_near,
    all_far,
    all_twin,
    sum_send,
    sum_near,
    sum_far,
    sum_twin,
):
    place = Place(lows, highs)
    count = place.count
    twin = (place.ep, 1 - place.tp)
    enter = place.greet()
    loads = [
        pltpu.make_async_copy(source, target, local_sems.at[i])
        for i, (source, target) in enumerate(
            (
                (query_weight, weights.at[0]),
                (key_weight, weights.at[1]),
                (value_weight, weights.at[2]),
                (gate_weight, weights.at[3]),
                (prior_state, state),
                (out_weight_far, out_weight),
                (shared_gate, sg),
                (shared_up, su),
                (shared_down, sd),
                (expert_gate.at[0], eg),
                (expert_up.at[0], eu),
                (expert_down.at[0], ed),
            )
        )
    ]
    for load in loads:
        load.start()
    seqs, model = tokens.shape
    half = model // 2
    width = out_weight.shape[1]
    projected, finish_first = project(
        place,
        enter,
        tokens,
        mix_gain,
        routes,
        route_gates,
        weights,
        loads[:4],
        gates_all,
        outgoing,
        features,
        first_part,
        first_landed,
        first_halfway,
        first_last,
        first_sems,
        first_send,
        first_near,
        first_far,
    )
    loads[4].wait()
    retained, rot_key = retain(place, projected, cosine, sine, state, turned, read)
    key_out[...] = rot_key
    value_out[...] = projected[2]
    held[place.lo, place.hi] = retained
    finish_held = gather_blocks(place, held, held_send, held_near, held_far)
    loads[5].wait()

    def multiply(l, carry):
        rows = held[l].reshape(highs * seqs, held.shape[3])
        piece = jnp.dot(rows, out_weight[...], preferred_element_type=F32).astype(BF16)
        columns[pl.ds(l * highs, highs)] = piece.reshape(highs, seqs, width)
        return carry

    lax.fori_loop(0, lows, multiply, 0)
    own_slot = place.tp * count + place.ep

    def send_back(i, carry):
        other = lax.rem(place.ep * 2 + place.tp + i, 2 * count)
        chip = other // 2
        slot = lax.rem(chip, lows) * highs + chip // lows
        start(
            columns.at[slot],
            mixed.at[own_slot],
            sems.at[0],
            sems.at[1],
            (chip, lax.rem(other, 2)),
        )
        return carry

    lax.fori_loop(1, 2 * count, send_back, 0)
    mixed[own_slot] = columns[place.lo * highs + place.hi]
    for load in loads[6:]:
        load.wait()
    drain(gates_all.at[pl.ds(0, count - 1)], first_sems.at[3])
    drain(mixed.at[pl.ds(0, 2 * count - 1)], sems.at[1])
    mixed_sum = jnp.concatenate(
        [(mixed[e].astype(F32) + mixed[count + e].astype(F32)) for e in range(count)], axis=1
    )
    mixed_sum = mixed_sum.astype(BF16).astype(F32)
    middle = tokens[...].astype(F32) + norm_rows(mixed_sum, post_gain[...])
    middle = middle.astype(BF16).astype(F32)
    moe_in = norm_rows(middle, ffn_gain[...]).astype(BF16)
    own_half = jnp.where(place.tp == 0, moe_in[:, :half], moe_in[:, half:])
    normed_all[place.tp, place.lo, place.hi] = own_half
    mine = normed_all.at[place.tp]

    def shared():
        shared_hidden = (
            jax.nn.silu(jnp.dot(moe_in, sg[...], preferred_element_type=F32))
            * jnp.dot(moe_in, su[...], preferred_element_type=F32)
        ).astype(BF16)
        shared_part = jnp.dot(shared_hidden, sd[...], preferred_element_type=F32).astype(BF16)
        for t in range(2):
            shared_pair[t] = shared_part[:, t * half : (t + 1) * half]
        start(shared_pair.at[1 - place.tp], shared_pair.at[2], sems.at[2], sems.at[3], twin)

    def hand_over(h):
        start(
            mine.at[:, h],
            normed_all.at[place.tp, :, h],
            sems.at[4],
            all_twin,
            twin,
        )

    finish_all = gather_blocks(place, mine, all_send, all_near, all_far, shared, hand_over)

    chunk = max(1, min(lows, 256 // (highs * seqs)))
    chunk_rows = chunk * highs * seqs
    steps = lows // chunk
    own_rows = pl.ds(pl.multiple_of(place.tp * half, half), half)
    other_rows = pl.ds(pl.multiple_of((1 - place.tp) * half, half), half)

    def near_half(i, carry):
        rows = normed_all[place.tp, pl.ds(i * chunk, chunk)].reshape(chunk_rows, half)
        gate_sum[i] = jnp.dot(rows, eg[own_rows, :], preferred_element_type=F32)
        up_sum[i] = jnp.dot(rows, eu[own_rows, :], preferred_element_type=F32)
        return carry

    lax.fori_loop(0, steps, near_half, 0)
    drain(normed_all.at[1 - place.tp], all_twin)

    def far_half(i, carry):
        rows = normed_all[1 - place.tp, pl.ds(i * chunk, chunk)].reshape(chunk_rows, half)
        gate_cols = gate_sum[i] + jnp.dot(rows, eg[other_rows, :], preferred_element_type=F32)
        up_cols = up_sum[i] + jnp.dot(rows, eu[other_rows, :], preferred_element_type=F32)
        hidden[i] = (jax.nn.silu(gate_cols) * up_cols).astype(BF16)
        return carry

    lax.fori_loop(0, steps, far_half, 0)
    cols = part.shape[4]

    def down(i, first):
        gate_rows = gates_all[pl.ds(i * chunk * highs, chunk * highs)].reshape(chunk_rows, count)
        lane = lax.broadcasted_iota(jnp.int32, (chunk_rows, count), 1)
        weight = jnp.sum(jnp.where(lane == place.ep, gate_rows, 0.0), axis=1, keepdims=True)
        span = pl.ds(pl.multiple_of(first, cols), cols)
        return jnp.dot(hidden[i], ed[:, span], preferred_element_type=F32) * weight

    for c in range(part.shape[0]):

        def outward(i, carry):
            piece = down(i, (1 - place.tp) * half + c * cols).astype(BF16)
            give[c, pl.ds(i * chunk, chunk)] = piece.reshape(chunk, highs, seqs, cols)
            return carry

        lax.fori_loop(0, steps, outward, 0)
        start(give.at[c], part.at[c], sems.at[5], sum_twin.at[c], twin)

    def fill(c):
        drain(part.at[c], sum_twin.at[c])

        def inward(i, carry):
            piece = down(i, place.tp * half + c * cols)
            other = part[c, pl.ds(i * chunk, chunk)].reshape(chunk_rows, cols).astype(F32)
            piece = (piece + other).astype(BF16)
            part[c, pl.ds(i * chunk, chunk)] = piece.reshape(chunk, highs, seqs, cols)
            return carry

        lax.fori_loop(0, steps, inward, 0)

    sums, finish_sums = scatter_sums(
        place, fill, part, landed, halfway, last, sum_send, sum_near, sum_far
    )
    drain(shared_pair.at[2], sems.at[3])
    pair[place.tp] = jnp.concatenate(sums, axis=1) + (
        shared_pair[place.tp].astype(F32) + shared_pair[2].astype(F32)
    )
    start(pair.at[place.tp], pair.at[place.tp], sems.at[6], sems.at[7], twin)
    drain(pair.at[1 - place.tp], sems.at[7])
    mixture = jnp.concatenate([pair[0], pair[1]], axis=1)
    result[...] = (middle + norm_rows(mixture, out_gain[...])).astype(BF16)
    finish_first()
    finish_held()
    finish_all()
    finish_sums()
    drain(mixed.at[pl.ds(0, 2 * count - 1)], sems.at[0])
    drain(shared_pair.at[2], sems.at[2])
    drain(mine, sems.at[4])
    drain(give, sems.at[5])
    drain(pair.at[0], sems.at[6])


VM = pl.BlockSpec(memory_space=pltpu.VMEM)
FAR = pl.BlockSpec(memory_space=pl.ANY)


def on_device(
    lows,
    highs,
    tokens,
    lengths,
    prior_state,
    mix_gain,
    post_gain,
    ffn_gain,
    out_gain,
    query_weight,
    key_weight,
    value_weight,
    gate_weight,
    out_weight,
    routes,
    route_gates,
    expert_gate,
    expert_up,
    expert_down,
    shared_gate,
    shared_up,
    shared_down,
):
    count = lows * highs
    seqs, model = tokens.shape
    width, local_cols = query_weight.shape
    heads_here = local_cols // HEAD
    hidden_cols = expert_gate.shape[2]
    shared_cols = shared_gate.shape[1]
    half = model // 2
    chunks = 4
    steps = lows // max(1, min(lows, 256 // (highs * seqs)))
    lane = jnp.arange(local_cols, dtype=jnp.int32)
    half_dim = HEAD // 2
    frequency = THETA ** (-(lane % half_dim).astype(F32) / half_dim)
    angles = lengths.astype(F32)[:, None] * frequency[None, :]
    cosine = jnp.cos(angles)
    sine = jnp.where((lane % HEAD < half_dim)[None, :], -jnp.sin(angles), jnp.sin(angles))
    result, rot_key, values = pl.pallas_call(
        functools.partial(layer_kernel, lows, highs),
        out_shape=(
            jax.ShapeDtypeStruct((seqs, model), BF16),
            jax.ShapeDtypeStruct((seqs, local_cols), F32),
            jax.ShapeDtypeStruct((seqs, local_cols), BF16),
        ),
        in_specs=[VM] * 9 + [FAR] * 12,
        out_specs=(VM, VM, VM),
        scratch_shapes=[
            pltpu.VMEM((4, width, local_cols), BF16),
            pltpu.VMEM((local_cols, width), BF16),
            pltpu.VMEM(prior_state.shape, F32),
            pltpu.VMEM((model, hidden_cols), BF16),
            pltpu.VMEM((model, hidden_cols), BF16),
            pltpu.VMEM((hidden_cols, model), BF16),
            pltpu.VMEM((model, shared_cols), BF16),
            pltpu.VMEM((model, shared_cols), BF16),
            pltpu.VMEM((shared_cols, model), BF16),
            pltpu.VMEM((count, seqs, count), F32),
            pltpu.VMEM((count, seqs, width), BF16),
            pltpu.VMEM((lows, highs, seqs, width), BF16),
            pltpu.VMEM((4, lows, highs, seqs, local_cols), BF16),
            pltpu.VMEM((4, lows, highs, seqs, local_cols), BF16),
            pltpu.VMEM((4, highs, seqs, local_cols), BF16),
            pltpu.VMEM((4, highs, seqs, local_cols), BF16),
            pltpu.VMEM((seqs, local_cols), F32),
            pltpu.VMEM((heads_here, seqs, HEAD), F32),
            pltpu.VMEM((lows, highs, seqs, local_cols), BF16),
            pltpu.VMEM((count, seqs, width), BF16),
            pltpu.VMEM((2 * count, seqs, width), BF16),
            pltpu.VMEM((2, lows, highs, seqs, half), BF16),
            pltpu.VMEM((steps, count * seqs // steps, hidden_cols), F32),
            pltpu.VMEM((steps, count * seqs // steps, hidden_cols), F32),
            pltpu.VMEM((steps, count * seqs // steps, hidden_cols), BF16),
            pltpu.VMEM((3, seqs, half), BF16),
            pltpu.VMEM((chunks, lows, highs, seqs, half // chunks), BF16),
            pltpu.VMEM((chunks, lows, highs, seqs, half // chunks), BF16),
            pltpu.VMEM((chunks, lows, highs, seqs, half // chunks), BF16),
            pltpu.VMEM((chunks, highs, seqs, half // chunks), BF16),
            pltpu.VMEM((chunks, highs, seqs, half // chunks), BF16),
            pltpu.VMEM((2, seqs, half), F32),
            pltpu.SemaphoreType.DMA((12,)),
            pltpu.SemaphoreType.DMA((8,)),
            pltpu.SemaphoreType.DMA((4,)),
            pltpu.SemaphoreType.DMA((2,)),
            pltpu.SemaphoreType.DMA((4,)),
            pltpu.SemaphoreType.DMA((4,)),
            pltpu.SemaphoreType.DMA((2,)),
            pltpu.SemaphoreType.DMA((highs,)),
            pltpu.SemaphoreType.DMA((highs,)),
            pltpu.SemaphoreType.DMA((2,)),
            pltpu.SemaphoreType.DMA((highs,)),
            pltpu.SemaphoreType.DMA((highs,)),
            pltpu.SemaphoreType.DMA,
            pltpu.SemaphoreType.DMA((2,)),
            pltpu.SemaphoreType.DMA((chunks,)),
            pltpu.SemaphoreType.DMA((chunks,)),
            pltpu.SemaphoreType.DMA((chunks,)),
        ],
        compiler_params=pltpu.CompilerParams(collective_id=0, has_side_effects=True),
        name="layer",
    )(
        tokens,
        cosine,
        sine,
        routes,
        route_gates,
        mix_gain.reshape(1, -1),
        post_gain.reshape(1, -1),
        ffn_gain.reshape(1, -1),
        out_gain.reshape(1, -1),
        prior_state,
        query_weight,
        key_weight,
        value_weight,
        gate_weight,
        out_weight,
        expert_gate,
        expert_up,
        expert_down,
        shared_gate,
        shared_up,
        shared_down,
    )
    decays = lax.dynamic_slice_in_dim(
        decay_table(HEADS), lax.axis_index("tp") * heads_here, heads_here, 0
    )
    layout = (seqs, heads_here, HEAD)
    new_state = (
        decays[None, :, None, None] * prior_state
        + rot_key.reshape(layout)[..., :, None] * values.astype(F32).reshape(layout)[..., None, :]
    )
    return (result, new_state)


def solution(mesh):
    count = mesh.shape["ep"]
    lows = 1
    while lows * lows < count:
        lows *= 2
    highs = count // lows
    return jax.shard_map(
        functools.partial(on_device, lows, highs),
        mesh=mesh,
        in_specs=(
            P("ep", None),
            P("ep"),
            P("ep", "tp", None, None),
            P(),
            P(),
            P(),
            P(),
            P("ep", "tp"),
            P("ep", "tp"),
            P("ep", "tp"),
            P("ep", "tp"),
            P("tp", "ep"),
            P("ep", None),
            P("ep", None),
            P("ep", None, "tp"),
            P("ep", None, "tp"),
            P("ep", "tp", None),
            P(None, "tp"),
            P(None, "tp"),
            P("tp", None),
        ),
        out_specs=(P("ep", None), P("ep", "tp", None, None)),
        check_vma=False,
    )
```

```python
import functools

import jax
import jax.numpy as jnp
from jax import lax
from jax.experimental import pallas as pl
from jax.experimental.pallas import tpu as pltpu
from jax.sharding import PartitionSpec as P

HEAD = 64
HEADS = 16
EPS = 1e-06
THETA = 10000.0
MESH = pl.DeviceIdType.MESH
F32 = jnp.float32
BF16 = jnp.bfloat16


def decay_table(head_count):
    head_order = jnp.arange(head_count, dtype=jnp.float32)
    return 1.0 - jnp.exp2(-5.0 - 7.0 * head_order / (head_count - 1))


def norm_rows(wide, gain):
    return wide * lax.rsqrt(jnp.mean(wide * wide, axis=-1, keepdims=True) + EPS) * gain


class Place:
    def __init__(self, lows, highs):
        self.lows, self.highs = lows, highs
        self.count = lows * highs
        self.ep = lax.axis_index("ep")
        self.tp = lax.axis_index("tp")
        self.hi = self.ep // lows
        self.lo = lax.rem(self.ep, lows)

    def greet(self):
        barrier = pltpu.get_barrier_semaphore()
        total = 2 * self.count
        flat = self.ep * 2 + self.tp

        def body(i, carry):
            other = lax.rem(flat + i, total)
            pl.semaphore_signal(
                barrier, inc=1, device_id=(other // 2, lax.rem(other, 2)), device_id_type=MESH
            )
            return carry

        lax.fori_loop(1, total, body, 0)
        return lambda: pl.semaphore_wait(barrier, total - 1)

    def all_peers(self, source_of, target, send, recv):
        def body(i, carry):
            other = lax.rem(self.ep + i, self.count)
            start(source_of(other), target, send, recv, (other, self.tp))
            return carry

        lax.fori_loop(1, self.count, body, 0)

    def low_peers(self, source_of, target, send, recv):
        def body(i, carry):
            other = lax.rem(self.lo + i, self.lows)
            start(source_of(other), target, send, recv, (self.hi * self.lows + other, self.tp))
            return carry

        lax.fori_loop(1, self.lows, body, 0)

    def high_peers(self, source_of, target, send, recv):
        def body(i, carry):
            other = lax.rem(self.hi + i, self.highs)
            start(source_of(other), target, send, recv, (other * self.lows + self.lo, self.tp))
            return carry

        lax.fori_loop(1, self.highs, body, 0)


def start(source, target, send, recv, device):
    pltpu.make_async_remote_copy(
        src_ref=source,
        dst_ref=target,
        send_sem=send,
        recv_sem=recv,
        device_id=device,
        device_id_type=MESH,
    ).start()


def drain(span, sem):
    pltpu.make_async_copy(span, span, sem).wait()


def gather_blocks(place, held, send, near, far, during=None, arrived=None):
    lows, highs = place.lows, place.highs
    own = held.at[place.lo, place.hi]
    place.high_peers(lambda other: own, own, send.at[0], far.at[place.hi])
    place.low_peers(lambda other: own, own, send.at[1], near.at[place.hi])
    if during is not None:
        during()
    for i in range(1, highs):
        h = lax.rem(place.hi + highs - i, highs)
        block = held.at[place.lo, h]
        drain(block, far.at[h])
        place.low_peers(lambda other: block, block, send.at[1], near.at[h])
    for i in range(highs):
        h = lax.rem(place.hi + highs - i, highs)
        drain(held.at[pl.ds(0, lows - 1), h], near.at[h])
        if arrived is not None:
            arrived(h)

    def finish():
        drain(held.at[0, pl.ds(0, highs - 1)], send.at[0])
        drain(held.at[pl.ds(0, lows - 1)], send.at[1])

    return finish


def scatter_sums(place, fill, part, landed, halfway, last, crossed, met, end, send, near, far):
    lows, highs = place.lows, place.highs
    plain = part.shape[0] - 1
    fill(plain)
    place.high_peers(
        lambda other: part.at[plain, :, other], crossed.at[place.hi], send.at[2], far.at[plain]
    )
    crossed[place.hi] = part[plain, :, place.hi]
    for c in range(plain):
        fill(c)
        place.low_peers(
            lambda other: part.at[c, other], landed.at[c, place.lo], send.at[0], near.at[c]
        )
        landed[c, place.lo] = part[c, place.lo]

    def low_first(c):
        drain(landed.at[c, pl.ds(0, lows - 1)], near.at[c])

        def fold(h, carry):
            total = landed[c, 0, h].astype(F32)
            for l in range(1, lows):
                total = total + landed[c, l, h].astype(F32)
            halfway[c, h] = total.astype(BF16)
            return carry

        lax.fori_loop(0, highs, fold, 0)
        place.high_peers(
            lambda other: halfway.at[c, other], last.at[c, place.hi], send.at[1], far.at[c]
        )
        last[c, place.hi] = halfway[c, place.hi]

    for c in range(plain - 1):
        low_first(c)
    drain(crossed.at[pl.ds(0, highs - 1)], far.at[plain])

    def fold_high(l, carry):
        total = crossed[0, l].astype(F32)
        for h in range(1, highs):
            total = total + crossed[h, l].astype(F32)
        met[l] = total.astype(BF16)
        return carry

    lax.fori_loop(0, lows, fold_high, 0)
    place.low_peers(lambda other: met.at[other], end.at[place.lo], send.at[3], near.at[plain])
    end[place.lo] = met[place.lo]
    low_first(plain - 1)
    sums = []
    for c in range(plain):
        drain(last.at[c, pl.ds(0, highs - 1)], far.at[c])
        total = last[c, 0].astype(F32)
        for h in range(1, highs):
            total = total + last[c, h].astype(F32)
        sums.append(total)
    drain(end.at[pl.ds(0, lows - 1)], near.at[plain])
    total = end[0].astype(F32)
    for l in range(1, lows):
        total = total + end[l].astype(F32)
    sums.append(total)

    def finish():
        drain(part.at[pl.ds(0, plain), pl.ds(0, lows - 1)], send.at[0])
        drain(halfway.at[:, pl.ds(0, highs - 1)], send.at[1])
        drain(crossed.at[pl.ds(0, highs - 1)], send.at[2])
        drain(met.at[pl.ds(0, lows - 1)], send.at[3])

    return sums, finish


def project(
    place,
    enter,
    tokens,
    gain,
    routes,
    route_gates,
    weights,
    weight_loads,
    gates_all,
    outgoing,
    features,
    part,
    landed,
    halfway,
    last,
    crossed,
    met,
    end,
    sems,
    send,
    near,
    far,
):
    lows, highs, count = place.lows, place.highs, place.count
    _, width, cols = weights.shape
    seqs = tokens.shape[0]
    normed = norm_rows(tokens[...].astype(F32), gain[...]).astype(BF16)
    for j in range(count):
        outgoing[j] = normed[:, j * width : (j + 1) * width]
    features[place.lo, place.hi] = outgoing[place.ep]
    expert = lax.broadcasted_iota(jnp.int32, (count, seqs), 0)
    dense = jnp.zeros((count, seqs), F32)
    for k in range(routes.shape[0]):
        dense = dense + jnp.where(expert == routes[k : k + 1, :], route_gates[k : k + 1, :], 0.0)
    own = place.lo * highs + place.hi
    gates_all[own] = dense.T
    with jax.named_scope("barrier"):
        enter()
    place.all_peers(
        lambda other: outgoing.at[other],
        features.at[place.lo, place.hi],
        sems.at[0],
        sems.at[1],
    )
    for load in weight_loads:
        load.wait()
    with jax.named_scope("wait_features"):
        drain(outgoing.at[pl.ds(0, count - 1)], sems.at[1])

    def fill(c):
        def multiply(l, carry):
            rows = features[l].reshape(highs * seqs, width)
            piece = jnp.dot(rows, weights[c], preferred_element_type=F32).astype(BF16)
            part[c, l] = piece.reshape(highs, seqs, cols)
            return carry

        lax.fori_loop(0, lows, multiply, 0)

    with jax.named_scope("sum_projections"):
        sums, finish = scatter_sums(
            place, fill, part, landed, halfway, last, crossed, met, end, send, near, far
        )
    place.all_peers(lambda other: gates_all.at[own], gates_all.at[own], sems.at[2], sems.at[3])

    def finish_all():
        finish()
        drain(outgoing.at[pl.ds(0, count - 1)], sems.at[0])
        drain(gates_all.at[pl.ds(0, count - 1)], sems.at[2])

    return [total.astype(BF16) for total in sums], finish_all


def head_sums(values):
    rows, cols = values.shape
    pair = 2 * HEAD
    row_of = lax.broadcasted_iota(jnp.int32, (pair, pair), 0) // HEAD
    col_of = lax.broadcasted_iota(jnp.int32, (pair, pair), 1) // HEAD
    ones = jnp.where(row_of == col_of, 1.0, 0.0).astype(F32)
    groups = cols // pair
    stacked = jnp.concatenate([values[:, g * pair : (g + 1) * pair] for g in range(groups)], axis=0)
    summed = jnp.dot(
        stacked, ones, preferred_element_type=F32, precision=lax.Precision.HIGHEST
    )
    return jnp.concatenate([summed[g * rows : (g + 1) * rows] for g in range(groups)], axis=1)


def retain(place, projected, cosine, sine, state, turned, read):
    queries, keys_new, values, out_gate = [member.astype(F32) for member in projected]
    seqs, cols = queries.shape
    lane = lax.broadcasted_iota(jnp.int32, (seqs, cols), 1)
    leading = lax.rem(lane, HEAD) < HEAD // 2

    def rotate(x):
        swapped = jnp.where(
            leading, pltpu.roll(x, cols - HEAD // 2, axis=1), pltpu.roll(x, HEAD // 2, axis=1)
        )
        return x * cosine[...] + swapped * sine[...]

    rot_query = rotate(queries)
    rot_key = rotate(keys_new) * HEAD ** (-0.5)
    turned[...] = rot_query
    pair = 2 * HEAD
    deep = lax.broadcasted_iota(jnp.int32, (HEAD, pair), 0)
    wide = lax.broadcasted_iota(jnp.int32, (HEAD, pair), 1)
    picks = [wide == deep, wide == deep + HEAD]

    def one_row(s, carry):
        row = turned[pl.ds(s, 1), :]
        for h in range(cols // HEAD):
            both = row[:, (h // 2) * pair : (h // 2 + 1) * pair]
            column = jnp.sum(
                jnp.where(picks[h % 2], jnp.broadcast_to(both, (HEAD, pair)), 0.0),
                axis=1,
                keepdims=True,
            )
            read[h, pl.ds(s, 1), :] = jnp.sum(column * state[s, h], axis=0, keepdims=True)
        return carry

    lax.fori_loop(0, seqs, one_row, 0)
    from_state = jnp.concatenate([read[h] for h in range(cols // HEAD)], axis=1)
    head = (place.tp * (cols // HEAD) + lane // HEAD).astype(F32)
    decays = 1.0 - jnp.exp2(-5.0 - 7.0 * head / (HEADS - 1))
    read_out = decays * from_state + head_sums(rot_query * rot_key) * values
    normed = read_out * lax.rsqrt(head_sums(read_out * read_out) / HEAD + EPS)
    return (normed * jax.nn.silu(out_gate)).astype(BF16), rot_key


def layer_kernel(
    lows,
    highs,
    tokens,
    cosine,
    sine,
    routes,
    route_gates,
    mix_gain,
    post_gain,
    ffn_gain,
    out_gain,
    prior_state,
    query_weight,
    key_weight,
    value_weight,
    gate_weight,
    out_weight_far,
    expert_gate,
    expert_up,
    expert_down,
    shared_gate,
    shared_up,
    shared_down,
    result,
    key_out,
    value_out,
    weights,
    out_weight,
    state,
    eg,
    eu,
    ed,
    sg,
    su,
    sd,
    gates_all,
    outgoing,
    features,
    first_part,
    first_landed,
    first_halfway,
    first_last,
    first_crossed,
    first_met,
    first_end,
    turned,
    read,
    held,
    columns,
    mixed,
    normed_all,
    gate_sum,
    up_sum,
    hidden,
    shared_pair,
    give,
    part,
    landed,
    halfway,
    last,
    crossed,
    met,
    end,
    pair,
    local_sems,
    sems,
    first_sems,
    first_send,
    first_near,
    first_far,
    held_send,
    held_near,
    held_far,
    all_send,
    all_near,
    all_far,
    all_twin,
    sum_send,
    sum_near,
    sum_far,
    sum_twin,
):
    place = Place(lows, highs)
    count = place.count
    twin = (place.ep, 1 - place.tp)
    enter = place.greet()
    loads = [
        pltpu.make_async_copy(source, target, local_sems.at[i])
        for i, (source, target) in enumerate(
            (
                (query_weight, weights.at[0]),
                (key_weight, weights.at[1]),
                (value_weight, weights.at[2]),
                (gate_weight, weights.at[3]),
                (prior_state, state),
                (out_weight_far, out_weight),
                (shared_gate, sg),
                (shared_up, su),
                (shared_down, sd),
                (expert_gate.at[0], eg),
                (expert_up.at[0], eu),
                (expert_down.at[0], ed),
            )
        )
    ]
    for load in loads:
        load.start()
    seqs, model = tokens.shape
    half = model // 2
    width = out_weight.shape[1]
    projected, finish_first = project(
        place,
        enter,
        tokens,
        mix_gain,
        routes,
        route_gates,
        weights,
        loads[:4],
        gates_all,
        outgoing,
        features,
        first_part,
        first_landed,
        first_halfway,
        first_last,
        first_crossed,
        first_met,
        first_end,
        first_sems,
        first_send,
        first_near,
        first_far,
    )
    loads[4].wait()
    with jax.named_scope("retain"):
        retained, rot_key = retain(place, projected, cosine, sine, state, turned, read)
        held[place.lo, place.hi] = retained

    def emit():
        values = projected[2].astype(F32)
        for h in range(key_out.shape[1]):
            key_out[:, h, :] = rot_key[:, h * HEAD : (h + 1) * HEAD]
            value_out[:, h, :] = values[:, h * HEAD : (h + 1) * HEAD]

    with jax.named_scope("gather_retained"):
        finish_held = gather_blocks(place, held, held_send, held_near, held_far, emit)
    loads[5].wait()

    def multiply(l, carry):
        rows = held[l].reshape(highs * seqs, held.shape[3])
        piece = jnp.dot(rows, out_weight[...], preferred_element_type=F32).astype(BF16)
        columns[pl.ds(l * highs, highs)] = piece.reshape(highs, seqs, width)
        return carry

    lax.fori_loop(0, lows, multiply, 0)
    own_slot = place.tp * count + place.ep

    def send_back(i, carry):
        other = lax.rem(place.ep * 2 + place.tp + i, 2 * count)
        chip = other // 2
        slot = lax.rem(chip, lows) * highs + chip // lows
        start(
            columns.at[slot],
            mixed.at[own_slot],
            sems.at[0],
            sems.at[1],
            (chip, lax.rem(other, 2)),
        )
        return carry

    lax.fori_loop(1, 2 * count, send_back, 0)
    mixed[own_slot] = columns[place.lo * highs + place.hi]
    for load in loads[6:]:
        load.wait()
    drain(gates_all.at[pl.ds(0, count - 1)], first_sems.at[3])
    with jax.named_scope("wait_mixed"):
        drain(mixed.at[pl.ds(0, 2 * count - 1)], sems.at[1])
    mixed_sum = jnp.concatenate(
        [(mixed[e].astype(F32) + mixed[count + e].astype(F32)) for e in range(count)], axis=1
    )
    mixed_sum = mixed_sum.astype(BF16).astype(F32)
    middle = tokens[...].astype(F32) + norm_rows(mixed_sum, post_gain[...])
    middle = middle.astype(BF16).astype(F32)
    moe_in = norm_rows(middle, ffn_gain[...]).astype(BF16)
    own_half = jnp.where(place.tp == 0, moe_in[:, :half], moe_in[:, half:])
    normed_all[place.tp, place.lo, place.hi] = own_half
    mine = normed_all.at[place.tp]

    def shared():
        shared_hidden = (
            jax.nn.silu(jnp.dot(moe_in, sg[...], preferred_element_type=F32))
            * jnp.dot(moe_in, su[...], preferred_element_type=F32)
        ).astype(BF16)
        shared_part = jnp.dot(shared_hidden, sd[...], preferred_element_type=F32).astype(BF16)
        for t in range(2):
            shared_pair[t] = shared_part[:, t * half : (t + 1) * half]
        start(shared_pair.at[1 - place.tp], shared_pair.at[2], sems.at[2], sems.at[3], twin)

    def hand_over(h):
        start(
            mine.at[:, h],
            normed_all.at[place.tp, :, h],
            sems.at[4],
            all_twin,
            twin,
        )

    with jax.named_scope("gather_moe"):
        finish_all = gather_blocks(place, mine, all_send, all_near, all_far, shared, hand_over)

    chunk = max(1, min(lows, 256 // (highs * seqs)))
    chunk_rows = chunk * highs * seqs
    steps = lows // chunk
    own_rows = pl.ds(pl.multiple_of(place.tp * half, half), half)
    other_rows = pl.ds(pl.multiple_of((1 - place.tp) * half, half), half)

    def near_half(i, carry):
        rows = normed_all[place.tp, pl.ds(i * chunk, chunk)].reshape(chunk_rows, half)
        gate_sum[i] = jnp.dot(rows, eg[own_rows, :], preferred_element_type=F32)
        up_sum[i] = jnp.dot(rows, eu[own_rows, :], preferred_element_type=F32)
        return carry

    with jax.named_scope("near_half"):
        lax.fori_loop(0, steps, near_half, 0)
    with jax.named_scope("wait_twin"):
        drain(normed_all.at[1 - place.tp], all_twin)

    def far_half(i, carry):
        rows = normed_all[1 - place.tp, pl.ds(i * chunk, chunk)].reshape(chunk_rows, half)
        gate_cols = gate_sum[i] + jnp.dot(rows, eg[other_rows, :], preferred_element_type=F32)
        up_cols = up_sum[i] + jnp.dot(rows, eu[other_rows, :], preferred_element_type=F32)
        hidden[i] = (jax.nn.silu(gate_cols) * up_cols).astype(BF16)
        return carry

    with jax.named_scope("far_half"):
        lax.fori_loop(0, steps, far_half, 0)
    cols = part.shape[4]

    def down(i, first):
        gate_rows = gates_all[pl.ds(i * chunk * highs, chunk * highs)].reshape(chunk_rows, count)
        lane = lax.broadcasted_iota(jnp.int32, (chunk_rows, count), 1)
        weight = jnp.sum(jnp.where(lane == place.ep, gate_rows, 0.0), axis=1, keepdims=True)
        span = pl.ds(pl.multiple_of(first, cols), cols)
        return jnp.dot(hidden[i], ed[:, span], preferred_element_type=F32) * weight

    for c in (part.shape[0] - 1, *range(part.shape[0] - 1)):

        def outward(i, carry):
            piece = down(i, (1 - place.tp) * half + c * cols).astype(BF16)
            give[c, pl.ds(i * chunk, chunk)] = piece.reshape(chunk, highs, seqs, cols)
            return carry

        lax.fori_loop(0, steps, outward, 0)
        start(give.at[c], part.at[c], sems.at[5], sum_twin.at[c], twin)

    def fill(c):
        drain(part.at[c], sum_twin.at[c])

        def inward(i, carry):
            piece = down(i, place.tp * half + c * cols)
            other = part[c, pl.ds(i * chunk, chunk)].reshape(chunk_rows, cols).astype(F32)
            piece = (piece + other).astype(BF16)
            part[c, pl.ds(i * chunk, chunk)] = piece.reshape(chunk, highs, seqs, cols)
            return carry

        lax.fori_loop(0, steps, inward, 0)

    with jax.named_scope("sum_experts"):
        sums, finish_sums = scatter_sums(
            place, fill, part, landed, halfway, last, crossed, met, end, sum_send, sum_near, sum_far
        )
    drain(shared_pair.at[2], sems.at[3])
    pair[place.tp] = jnp.concatenate(sums, axis=1) + (
        shared_pair[place.tp].astype(F32) + shared_pair[2].astype(F32)
    )
    start(pair.at[place.tp], pair.at[place.tp], sems.at[6], sems.at[7], twin)
    with jax.named_scope("wait_pair"):
        drain(pair.at[1 - place.tp], sems.at[7])
    mixture = jnp.concatenate([pair[0], pair[1]], axis=1)
    result[...] = (middle + norm_rows(mixture, out_gain[...])).astype(BF16)
    finish_first()
    finish_held()
    finish_all()
    finish_sums()
    drain(mixed.at[pl.ds(0, 2 * count - 1)], sems.at[0])
    drain(shared_pair.at[2], sems.at[2])
    drain(mine, sems.at[4])
    drain(give, sems.at[5])
    drain(pair.at[0], sems.at[6])


VM = pl.BlockSpec(memory_space=pltpu.VMEM)
FAR = pl.BlockSpec(memory_space=pl.ANY)


def on_device(
    lows,
    highs,
    tokens,
    lengths,
    prior_state,
    mix_gain,
    post_gain,
    ffn_gain,
    out_gain,
    query_weight,
    key_weight,
    value_weight,
    gate_weight,
    out_weight,
    routes,
    route_gates,
    expert_gate,
    expert_up,
    expert_down,
    shared_gate,
    shared_up,
    shared_down,
):
    count = lows * highs
    seqs, model = tokens.shape
    width, local_cols = query_weight.shape
    heads_here = local_cols // HEAD
    hidden_cols = expert_gate.shape[2]
    shared_cols = shared_gate.shape[1]
    half = model // 2
    chunks = 4
    steps = lows // max(1, min(lows, 256 // (highs * seqs)))
    lane = jnp.arange(local_cols, dtype=jnp.int32)
    half_dim = HEAD // 2
    frequency = THETA ** (-(lane % half_dim).astype(F32) / half_dim)
    angles = lengths.astype(F32)[:, None] * frequency[None, :]
    cosine = jnp.cos(angles)
    sine = jnp.where((lane % HEAD < half_dim)[None, :], -jnp.sin(angles), jnp.sin(angles))
    result, rot_key, values = pl.pallas_call(
        functools.partial(layer_kernel, lows, highs),
        out_shape=(
            jax.ShapeDtypeStruct((seqs, model), BF16),
            jax.ShapeDtypeStruct((seqs, heads_here, HEAD), F32),
            jax.ShapeDtypeStruct((seqs, heads_here, HEAD), F32),
        ),
        in_specs=[VM] * 9 + [FAR] * 12,
        out_specs=(VM, VM, VM),
        scratch_shapes=[
            pltpu.VMEM((4, width, local_cols), BF16),
            pltpu.VMEM((local_cols, width), BF16),
            pltpu.VMEM(prior_state.shape, F32),
            pltpu.VMEM((model, hidden_cols), BF16),
            pltpu.VMEM((model, hidden_cols), BF16),
            pltpu.VMEM((hidden_cols, model), BF16),
            pltpu.VMEM((model, shared_cols), BF16),
            pltpu.VMEM((model, shared_cols), BF16),
            pltpu.VMEM((shared_cols, model), BF16),
            pltpu.VMEM((count, seqs, count), F32),
            pltpu.VMEM((count, seqs, width), BF16),
            pltpu.VMEM((lows, highs, seqs, width), BF16),
            pltpu.VMEM((4, lows, highs, seqs, local_cols), BF16),
            pltpu.VMEM((3, lows, highs, seqs, local_cols), BF16),
            pltpu.VMEM((3, highs, seqs, local_cols), BF16),
            pltpu.VMEM((3, highs, seqs, local_cols), BF16),
            pltpu.VMEM((highs, lows, seqs, local_cols), BF16),
            pltpu.VMEM((lows, seqs, local_cols), BF16),
            pltpu.VMEM((lows, seqs, local_cols), BF16),
            pltpu.VMEM((seqs, local_cols), F32),
            pltpu.VMEM((heads_here, seqs, HEAD), F32),
            pltpu.VMEM((lows, highs, seqs, local_cols), BF16),
            pltpu.VMEM((count, seqs, width), BF16),
            pltpu.VMEM((2 * count, seqs, width), BF16),
            pltpu.VMEM((2, lows, highs, seqs, half), BF16),
            pltpu.VMEM((steps, count * seqs // steps, hidden_cols), F32),
            pltpu.VMEM((steps, count * seqs // steps, hidden_cols), F32),
            pltpu.VMEM((steps, count * seqs // steps, hidden_cols), BF16),
            pltpu.VMEM((3, seqs, half), BF16),
            pltpu.VMEM((chunks, lows, highs, seqs, half // chunks), BF16),
            pltpu.VMEM((chunks, lows, highs, seqs, half // chunks), BF16),
            pltpu.VMEM((chunks - 1, lows, highs, seqs, half // chunks), BF16),
            pltpu.VMEM((chunks - 1, highs, seqs, half // chunks), BF16),
            pltpu.VMEM((chunks - 1, highs, seqs, half // chunks), BF16),
            pltpu.VMEM((highs, lows, seqs, half // chunks), BF16),
            pltpu.VMEM((lows, seqs, half // chunks), BF16),
            pltpu.VMEM((lows, seqs, half // chunks), BF16),
            pltpu.VMEM((2, seqs, half), F32),
            pltpu.SemaphoreType.DMA((12,)),
            pltpu.SemaphoreType.DMA((8,)),
            pltpu.SemaphoreType.DMA((4,)),
            pltpu.SemaphoreType.DMA((4,)),
            pltpu.SemaphoreType.DMA((4,)),
            pltpu.SemaphoreType.DMA((4,)),
            pltpu.SemaphoreType.DMA((2,)),
            pltpu.SemaphoreType.DMA((highs,)),
            pltpu.SemaphoreType.DMA((highs,)),
            pltpu.SemaphoreType.DMA((2,)),
            pltpu.SemaphoreType.DMA((highs,)),
            pltpu.SemaphoreType.DMA((highs,)),
            pltpu.SemaphoreType.DMA,
            pltpu.SemaphoreType.DMA((4,)),
            pltpu.SemaphoreType.DMA((chunks,)),
            pltpu.SemaphoreType.DMA((chunks,)),
            pltpu.SemaphoreType.DMA((chunks,)),
        ],
        compiler_params=pltpu.CompilerParams(collective_id=0, has_side_effects=True),
        name="layer",
    )(
        tokens,
        cosine,
        sine,
        routes.T,
        route_gates.T,
        mix_gain.reshape(1, -1),
        post_gain.reshape(1, -1),
        ffn_gain.reshape(1, -1),
        out_gain.reshape(1, -1),
        prior_state,
        query_weight,
        key_weight,
        value_weight,
        gate_weight,
        out_weight,
        expert_gate,
        expert_up,
        expert_down,
        shared_gate,
        shared_up,
        shared_down,
    )
    decays = lax.dynamic_slice_in_dim(
        decay_table(HEADS), lax.axis_index("tp") * heads_here, heads_here, 0
    )
    new_state = (
        decays[None, :, None, None] * prior_state
        + rot_key[..., :, None] * values[..., None, :]
    )
    return (result, new_state)


def solution(mesh):
    count = mesh.shape["ep"]
    lows = 1
    while lows * lows < count:
        lows *= 2
    highs = count // lows
    return jax.shard_map(
        functools.partial(on_device, lows, highs),
        mesh=mesh,
        in_specs=(
            P("ep", None),
            P("ep"),
            P("ep", "tp", None, None),
            P(),
            P(),
            P(),
            P(),
            P("ep", "tp"),
            P("ep", "tp"),
            P("ep", "tp"),
            P("ep", "tp"),
            P("tp", "ep"),
            P("ep", None),
            P("ep", None),
            P("ep", None, "tp"),
            P("ep", None, "tp"),
            P("ep", "tp", None),
            P(None, "tp"),
            P(None, "tp"),
            P("tp", None),
        ),
        out_specs=(P("ep", None), P("ep", "tp", None, None)),
        check_vma=False,
    )
```

```python
import functools

import jax
import jax.numpy as jnp
from jax import lax
from jax.experimental import pallas as pl
from jax.experimental.pallas import tpu as pltpu
from jax.sharding import PartitionSpec as P

HEAD = 64
HEADS = 16
EPS = 1e-06
THETA = 10000.0
MESH = pl.DeviceIdType.MESH
F32 = jnp.float32
BF16 = jnp.bfloat16


def decay_table(head_count):
    head_order = jnp.arange(head_count, dtype=jnp.float32)
    return 1.0 - jnp.exp2(-5.0 - 7.0 * head_order / (head_count - 1))


def norm_rows(wide, gain):
    return wide * lax.rsqrt(jnp.mean(wide * wide, axis=-1, keepdims=True) + EPS) * gain


class Place:
    def __init__(self, lows, highs):
        self.lows, self.highs = lows, highs
        self.count = lows * highs
        self.ep = lax.axis_index("ep")
        self.tp = lax.axis_index("tp")
        self.hi = self.ep // lows
        self.lo = lax.rem(self.ep, lows)

    def greet(self):
        barrier = pltpu.get_barrier_semaphore()
        total = 2 * self.count
        flat = self.ep * 2 + self.tp

        def body(i, carry):
            other = lax.rem(flat + i, total)
            pl.semaphore_signal(
                barrier, inc=1, device_id=(other // 2, lax.rem(other, 2)), device_id_type=MESH
            )
            return carry

        lax.fori_loop(1, total, body, 0)
        return lambda: pl.semaphore_wait(barrier, total - 1)

    def all_peers(self, source_of, target, send, recv):
        def body(i, carry):
            other = lax.rem(self.ep + i, self.count)
            start(source_of(other), target, send, recv, (other, self.tp))
            return carry

        lax.fori_loop(1, self.count, body, 0)

    def low_peers(self, source_of, target, send, recv):
        def body(i, carry):
            other = lax.rem(self.lo + i, self.lows)
            start(source_of(other), target, send, recv, (self.hi * self.lows + other, self.tp))
            return carry

        lax.fori_loop(1, self.lows, body, 0)

    def high_peers(self, source_of, target, send, recv):
        def body(i, carry):
            other = lax.rem(self.hi + i, self.highs)
            start(source_of(other), target, send, recv, (other * self.lows + self.lo, self.tp))
            return carry

        lax.fori_loop(1, self.highs, body, 0)


def start(source, target, send, recv, device):
    pltpu.make_async_remote_copy(
        src_ref=source,
        dst_ref=target,
        send_sem=send,
        recv_sem=recv,
        device_id=device,
        device_id_type=MESH,
    ).start()


def drain(span, sem):
    pltpu.make_async_copy(span, span, sem).wait()


def gather_blocks(place, held, send, near, far, during=None, arrived=None):
    lows, highs = place.lows, place.highs
    own = held.at[place.lo, place.hi]
    place.high_peers(lambda other: own, own, send.at[0], far.at[place.hi])
    place.low_peers(lambda other: own, own, send.at[1], near.at[place.hi])
    if during is not None:
        during()
    for i in range(1, highs):
        h = lax.rem(place.hi + highs - i, highs)
        block = held.at[place.lo, h]
        drain(block, far.at[h])
        place.low_peers(lambda other: block, block, send.at[1], near.at[h])
    for i in range(highs):
        h = lax.rem(place.hi + highs - i, highs)
        drain(held.at[pl.ds(0, lows - 1), h], near.at[h])
        if arrived is not None:
            arrived(h)

    def finish():
        drain(held.at[0, pl.ds(0, highs - 1)], send.at[0])
        drain(held.at[pl.ds(0, lows - 1)], send.at[1])

    return finish


def scatter_sums(place, fill, part, landed, halfway, last, crossed, met, end, send, near, far):
    lows, highs = place.lows, place.highs
    plain = part.shape[0] - 1
    fill(plain)
    place.high_peers(
        lambda other: part.at[plain, :, other], crossed.at[place.hi], send.at[2], far.at[plain]
    )
    crossed[place.hi] = part[plain, :, place.hi]
    for c in range(plain):
        fill(c)
        place.low_peers(
            lambda other: part.at[c, other], landed.at[c, place.lo], send.at[0], near.at[c]
        )
        landed[c, place.lo] = part[c, place.lo]

    def low_first(c):
        drain(landed.at[c, pl.ds(0, lows - 1)], near.at[c])

        def fold(h, carry):
            total = landed[c, 0, h].astype(F32)
            for l in range(1, lows):
                total = total + landed[c, l, h].astype(F32)
            halfway[c, h] = total.astype(BF16)
            return carry

        lax.fori_loop(0, highs, fold, 0)
        place.high_peers(
            lambda other: halfway.at[c, other], last.at[c, place.hi], send.at[1], far.at[c]
        )
        last[c, place.hi] = halfway[c, place.hi]

    for c in range(plain - 1):
        low_first(c)
    drain(crossed.at[pl.ds(0, highs - 1)], far.at[plain])

    def fold_high(l, carry):
        total = crossed[0, l].astype(F32)
        for h in range(1, highs):
            total = total + crossed[h, l].astype(F32)
        met[l] = total.astype(BF16)
        return carry

    lax.fori_loop(0, lows, fold_high, 0)
    place.low_peers(lambda other: met.at[other], end.at[place.lo], send.at[3], near.at[plain])
    end[place.lo] = met[place.lo]
    low_first(plain - 1)
    sums = []
    for c in range(plain):
        drain(last.at[c, pl.ds(0, highs - 1)], far.at[c])
        total = last[c, 0].astype(F32)
        for h in range(1, highs):
            total = total + last[c, h].astype(F32)
        sums.append(total)
    drain(end.at[pl.ds(0, lows - 1)], near.at[plain])
    total = end[0].astype(F32)
    for l in range(1, lows):
        total = total + end[l].astype(F32)
    sums.append(total)

    def finish():
        drain(part.at[pl.ds(0, plain), pl.ds(0, lows - 1)], send.at[0])
        drain(halfway.at[:, pl.ds(0, highs - 1)], send.at[1])
        drain(crossed.at[pl.ds(0, highs - 1)], send.at[2])
        drain(met.at[pl.ds(0, lows - 1)], send.at[3])

    return sums, finish


def project(
    place,
    enter,
    tokens,
    gain,
    routes,
    route_gates,
    weights,
    weight_loads,
    gates_all,
    outgoing,
    features,
    part,
    landed,
    halfway,
    last,
    crossed,
    met,
    end,
    sems,
    send,
    near,
    far,
):
    lows, highs, count = place.lows, place.highs, place.count
    _, width, cols = weights.shape
    seqs = tokens.shape[0]
    normed = norm_rows(tokens[...].astype(F32), gain[...]).astype(BF16)
    for j in range(count):
        outgoing[j] = normed[:, j * width : (j + 1) * width]
    features[place.lo, place.hi] = outgoing[place.ep]
    expert = lax.broadcasted_iota(jnp.int32, (count, seqs), 0)
    dense = jnp.zeros((count, seqs), F32)
    for k in range(routes.shape[0]):
        dense = dense + jnp.where(expert == routes[k : k + 1, :], route_gates[k : k + 1, :], 0.0)
    own = place.lo * highs + place.hi
    gates_all[own] = dense.T
    with jax.named_scope("barrier"):
        enter()
    place.all_peers(
        lambda other: outgoing.at[other],
        features.at[place.lo, place.hi],
        sems.at[0],
        sems.at[1],
    )
    for load in weight_loads:
        load.wait()
    with jax.named_scope("wait_features"):
        drain(outgoing.at[pl.ds(0, count - 1)], sems.at[1])

    def fill(c):
        def multiply(l, carry):
            rows = features[l].reshape(highs * seqs, width)
            piece = jnp.dot(rows, weights[c], preferred_element_type=F32).astype(BF16)
            part[c, l] = piece.reshape(highs, seqs, cols)
            return carry

        lax.fori_loop(0, lows, multiply, 0)

    with jax.named_scope("sum_projections"):
        sums, finish = scatter_sums(
            place, fill, part, landed, halfway, last, crossed, met, end, send, near, far
        )
    place.all_peers(lambda other: gates_all.at[own], gates_all.at[own], sems.at[2], sems.at[3])

    def finish_all():
        finish()
        drain(outgoing.at[pl.ds(0, count - 1)], sems.at[0])
        drain(gates_all.at[pl.ds(0, count - 1)], sems.at[2])

    return [total.astype(BF16) for total in sums], finish_all


def head_sums(values):
    rows, cols = values.shape
    pair = 2 * HEAD
    row_of = lax.broadcasted_iota(jnp.int32, (pair, pair), 0) // HEAD
    col_of = lax.broadcasted_iota(jnp.int32, (pair, pair), 1) // HEAD
    ones = jnp.where(row_of == col_of, 1.0, 0.0).astype(F32)
    groups = cols // pair
    stacked = jnp.concatenate([values[:, g * pair : (g + 1) * pair] for g in range(groups)], axis=0)
    summed = jnp.dot(
        stacked, ones, preferred_element_type=F32, precision=lax.Precision.HIGHEST
    )
    return jnp.concatenate([summed[g * rows : (g + 1) * rows] for g in range(groups)], axis=1)


def retain(place, projected, cosine, sine, state, turned, read):
    queries, keys_new, values, out_gate = [member.astype(F32) for member in projected]
    seqs, cols = queries.shape
    lane = lax.broadcasted_iota(jnp.int32, (seqs, cols), 1)
    leading = lax.rem(lane, HEAD) < HEAD // 2

    def rotate(x):
        swapped = jnp.where(
            leading, pltpu.roll(x, cols - HEAD // 2, axis=1), pltpu.roll(x, HEAD // 2, axis=1)
        )
        return x * cosine[...] + swapped * sine[...]

    rot_query = rotate(queries)
    rot_key = rotate(keys_new) * HEAD ** (-0.5)
    turned[...] = rot_query
    pair = 2 * HEAD
    deep = lax.broadcasted_iota(jnp.int32, (HEAD, pair), 0)
    wide = lax.broadcasted_iota(jnp.int32, (HEAD, pair), 1)
    picks = [wide == deep, wide == deep + HEAD]

    together = 4

    def some_rows(i, carry):
        for s in [i * together + u for u in range(together)]:
            row = turned[pl.ds(s, 1), :]
            for h in range(cols // HEAD):
                both = row[:, (h // 2) * pair : (h // 2 + 1) * pair]
                column = jnp.sum(
                    jnp.where(picks[h % 2], jnp.broadcast_to(both, (HEAD, pair)), 0.0),
                    axis=1,
                    keepdims=True,
                )
                read[h, pl.ds(s, 1), :] = jnp.sum(column * state[s, h], axis=0, keepdims=True)
        return carry

    lax.fori_loop(0, seqs // together, some_rows, 0)
    from_state = jnp.concatenate([read[h] for h in range(cols // HEAD)], axis=1)
    head = (place.tp * (cols // HEAD) + lane // HEAD).astype(F32)
    decays = 1.0 - jnp.exp2(-5.0 - 7.0 * head / (HEADS - 1))
    read_out = decays * from_state + head_sums(rot_query * rot_key) * values
    normed = read_out * lax.rsqrt(head_sums(read_out * read_out) / HEAD + EPS)
    return (normed * jax.nn.silu(out_gate)).astype(BF16), rot_key


def layer_kernel(
    lows,
    highs,
    tokens,
    cosine,
    sine,
    routes,
    route_gates,
    mix_gain,
    post_gain,
    ffn_gain,
    out_gain,
    prior_state,
    query_weight,
    key_weight,
    value_weight,
    gate_weight,
    out_weight_far,
    expert_gate,
    expert_up,
    expert_down,
    shared_gate,
    shared_up,
    shared_down,
    result,
    key_out,
    value_out,
    weights,
    out_weight,
    state,
    eg,
    eu,
    ed,
    sg,
    su,
    sd,
    gates_all,
    outgoing,
    features,
    first_part,
    first_landed,
    first_halfway,
    first_last,
    first_crossed,
    first_met,
    first_end,
    turned,
    read,
    held,
    columns,
    mixed,
    normed_all,
    gate_sum,
    up_sum,
    hidden,
    shared_pair,
    give,
    part,
    landed,
    halfway,
    last,
    crossed,
    met,
    end,
    pair,
    local_sems,
    sems,
    first_sems,
    first_send,
    first_near,
    first_far,
    held_send,
    held_near,
    held_far,
    all_send,
    all_near,
    all_far,
    all_twin,
    sum_send,
    sum_near,
    sum_far,
    sum_twin,
):
    place = Place(lows, highs)
    count = place.count
    twin = (place.ep, 1 - place.tp)
    enter = place.greet()
    loads = [
        pltpu.make_async_copy(source, target, local_sems.at[i])
        for i, (source, target) in enumerate(
            (
                (query_weight, weights.at[0]),
                (key_weight, weights.at[1]),
                (value_weight, weights.at[2]),
                (gate_weight, weights.at[3]),
                (prior_state, state),
                (out_weight_far, out_weight),
                (shared_gate, sg),
                (shared_up, su),
                (shared_down, sd),
                (expert_gate.at[0], eg),
                (expert_up.at[0], eu),
                (expert_down.at[0], ed),
            )
        )
    ]
    for load in loads:
        load.start()
    seqs, model = tokens.shape
    half = model // 2
    width = out_weight.shape[1]
    projected, finish_first = project(
        place,
        enter,
        tokens,
        mix_gain,
        routes,
        route_gates,
        weights,
        loads[:4],
        gates_all,
        outgoing,
        features,
        first_part,
        first_landed,
        first_halfway,
        first_last,
        first_crossed,
        first_met,
        first_end,
        first_sems,
        first_send,
        first_near,
        first_far,
    )
    loads[4].wait()
    with jax.named_scope("retain"):
        retained, rot_key = retain(place, projected, cosine, sine, state, turned, read)
        held[place.lo, place.hi] = retained

    def emit():
        values = projected[2].astype(F32)
        for h in range(key_out.shape[1]):
            key_out[:, h, :] = rot_key[:, h * HEAD : (h + 1) * HEAD]
            value_out[:, h, :] = values[:, h * HEAD : (h + 1) * HEAD]

    with jax.named_scope("gather_retained"):
        finish_held = gather_blocks(place, held, held_send, held_near, held_far, emit)
    loads[5].wait()

    def multiply(l, carry):
        rows = held[l].reshape(highs * seqs, held.shape[3])
        piece = jnp.dot(rows, out_weight[...], preferred_element_type=F32).astype(BF16)
        columns[pl.ds(l * highs, highs)] = piece.reshape(highs, seqs, width)
        return carry

    lax.fori_loop(0, lows, multiply, 0)
    own_slot = place.tp * count + place.ep

    def send_back(i, carry):
        other = lax.rem(place.ep * 2 + place.tp + i, 2 * count)
        chip = other // 2
        slot = lax.rem(chip, lows) * highs + chip // lows
        start(
            columns.at[slot],
            mixed.at[own_slot],
            sems.at[0],
            sems.at[1],
            (chip, lax.rem(other, 2)),
        )
        return carry

    lax.fori_loop(1, 2 * count, send_back, 0)
    mixed[own_slot] = columns[place.lo * highs + place.hi]
    for load in loads[6:]:
        load.wait()
    drain(gates_all.at[pl.ds(0, count - 1)], first_sems.at[3])
    with jax.named_scope("wait_mixed"):
        drain(mixed.at[pl.ds(0, 2 * count - 1)], sems.at[1])
    mixed_sum = jnp.concatenate(
        [(mixed[e].astype(F32) + mixed[count + e].astype(F32)) for e in range(count)], axis=1
    )
    mixed_sum = mixed_sum.astype(BF16).astype(F32)
    middle = tokens[...].astype(F32) + norm_rows(mixed_sum, post_gain[...])
    middle = middle.astype(BF16).astype(F32)
    moe_in = norm_rows(middle, ffn_gain[...]).astype(BF16)
    own_half = jnp.where(place.tp == 0, moe_in[:, :half], moe_in[:, half:])
    normed_all[place.tp, place.lo, place.hi] = own_half
    mine = normed_all.at[place.tp]

    def shared():
        shared_hidden = (
            jax.nn.silu(jnp.dot(moe_in, sg[...], preferred_element_type=F32))
            * jnp.dot(moe_in, su[...], preferred_element_type=F32)
        ).astype(BF16)
        shared_part = jnp.dot(shared_hidden, sd[...], preferred_element_type=F32).astype(BF16)
        for t in range(2):
            shared_pair[t] = shared_part[:, t * half : (t + 1) * half]
        start(shared_pair.at[1 - place.tp], shared_pair.at[2], sems.at[2], sems.at[3], twin)

    def hand_over(h):
        start(
            mine.at[:, h],
            normed_all.at[place.tp, :, h],
            sems.at[4],
            all_twin,
            twin,
        )

    with jax.named_scope("gather_moe"):
        finish_all = gather_blocks(place, mine, all_send, all_near, all_far, shared, hand_over)

    chunk = max(1, min(lows, 256 // (highs * seqs)))
    chunk_rows = chunk * highs * seqs
    steps = lows // chunk
    own_rows = pl.ds(pl.multiple_of(place.tp * half, half), half)
    other_rows = pl.ds(pl.multiple_of((1 - place.tp) * half, half), half)

    def near_half(i, carry):
        rows = normed_all[place.tp, pl.ds(i * chunk, chunk)].reshape(chunk_rows, half)
        gate_sum[i] = jnp.dot(rows, eg[own_rows, :], preferred_element_type=F32)
        up_sum[i] = jnp.dot(rows, eu[own_rows, :], preferred_element_type=F32)
        return carry

    with jax.named_scope("near_half"):
        lax.fori_loop(0, steps, near_half, 0)
    with jax.named_scope("wait_twin"):
        drain(normed_all.at[1 - place.tp], all_twin)

    def far_half(i, carry):
        rows = normed_all[1 - place.tp, pl.ds(i * chunk, chunk)].reshape(chunk_rows, half)
        gate_cols = gate_sum[i] + jnp.dot(rows, eg[other_rows, :], preferred_element_type=F32)
        up_cols = up_sum[i] + jnp.dot(rows, eu[other_rows, :], preferred_element_type=F32)
        hidden[i] = (jax.nn.silu(gate_cols) * up_cols).astype(BF16)
        return carry

    with jax.named_scope("far_half"):
        lax.fori_loop(0, steps, far_half, 0)
    cols = part.shape[4]

    def down(i, first):
        gate_rows = gates_all[pl.ds(i * chunk * highs, chunk * highs)].reshape(chunk_rows, count)
        lane = lax.broadcasted_iota(jnp.int32, (chunk_rows, count), 1)
        weight = jnp.sum(jnp.where(lane == place.ep, gate_rows, 0.0), axis=1, keepdims=True)
        span = pl.ds(pl.multiple_of(first, cols), cols)
        return jnp.dot(hidden[i], ed[:, span], preferred_element_type=F32) * weight

    for c in (part.shape[0] - 1, *range(part.shape[0] - 1)):

        def outward(i, carry):
            piece = down(i, (1 - place.tp) * half + c * cols).astype(BF16)
            give[c, pl.ds(i * chunk, chunk)] = piece.reshape(chunk, highs, seqs, cols)
            return carry

        lax.fori_loop(0, steps, outward, 0)
        start(give.at[c], part.at[c], sems.at[5], sum_twin.at[c], twin)

    def fill(c):
        drain(part.at[c], sum_twin.at[c])

        def inward(i, carry):
            piece = down(i, place.tp * half + c * cols)
            other = part[c, pl.ds(i * chunk, chunk)].reshape(chunk_rows, cols).astype(F32)
            piece = (piece + other).astype(BF16)
            part[c, pl.ds(i * chunk, chunk)] = piece.reshape(chunk, highs, seqs, cols)
            return carry

        lax.fori_loop(0, steps, inward, 0)

    with jax.named_scope("sum_experts"):
        sums, finish_sums = scatter_sums(
            place, fill, part, landed, halfway, last, crossed, met, end, sum_send, sum_near, sum_far
        )
    drain(shared_pair.at[2], sems.at[3])
    pair[place.tp] = jnp.concatenate(sums, axis=1) + (
        shared_pair[place.tp].astype(F32) + shared_pair[2].astype(F32)
    )
    start(pair.at[place.tp], pair.at[place.tp], sems.at[6], sems.at[7], twin)
    with jax.named_scope("wait_pair"):
        drain(pair.at[1 - place.tp], sems.at[7])
    mixture = jnp.concatenate([pair[0], pair[1]], axis=1)
    result[...] = (middle + norm_rows(mixture, out_gain[...])).astype(BF16)
    finish_first()
    finish_held()
    finish_all()
    finish_sums()
    drain(mixed.at[pl.ds(0, 2 * count - 1)], sems.at[0])
    drain(shared_pair.at[2], sems.at[2])
    drain(mine, sems.at[4])
    drain(give, sems.at[5])
    drain(pair.at[0], sems.at[6])


VM = pl.BlockSpec(memory_space=pltpu.VMEM)
FAR = pl.BlockSpec(memory_space=pl.ANY)


def on_device(
    lows,
    highs,
    tokens,
    lengths,
    prior_state,
    mix_gain,
    post_gain,
    ffn_gain,
    out_gain,
    query_weight,
    key_weight,
    value_weight,
    gate_weight,
    out_weight,
    routes,
    route_gates,
    expert_gate,
    expert_up,
    expert_down,
    shared_gate,
    shared_up,
    shared_down,
):
    count = lows * highs
    seqs, model = tokens.shape
    width, local_cols = query_weight.shape
    heads_here = local_cols // HEAD
    hidden_cols = expert_gate.shape[2]
    shared_cols = shared_gate.shape[1]
    half = model // 2
    chunks = 4
    steps = lows // max(1, min(lows, 256 // (highs * seqs)))
    lane = jnp.arange(local_cols, dtype=jnp.int32)
    half_dim = HEAD // 2
    frequency = THETA ** (-(lane % half_dim).astype(F32) / half_dim)
    angles = lengths.astype(F32)[:, None] * frequency[None, :]
    cosine = jnp.cos(angles)
    sine = jnp.where((lane % HEAD < half_dim)[None, :], -jnp.sin(angles), jnp.sin(angles))
    result, rot_key, values = pl.pallas_call(
        functools.partial(layer_kernel, lows, highs),
        out_shape=(
            jax.ShapeDtypeStruct((seqs, model), BF16),
            jax.ShapeDtypeStruct((seqs, heads_here, HEAD), F32),
            jax.ShapeDtypeStruct((seqs, heads_here, HEAD), F32),
        ),
        in_specs=[VM] * 9 + [FAR] * 12,
        out_specs=(VM, VM, VM),
        scratch_shapes=[
            pltpu.VMEM((4, width, local_cols), BF16),
            pltpu.VMEM((local_cols, width), BF16),
            pltpu.VMEM(prior_state.shape, F32),
            pltpu.VMEM((model, hidden_cols), BF16),
            pltpu.VMEM((model, hidden_cols), BF16),
            pltpu.VMEM((hidden_cols, model), BF16),
            pltpu.VMEM((model, shared_cols), BF16),
            pltpu.VMEM((model, shared_cols), BF16),
            pltpu.VMEM((shared_cols, model), BF16),
            pltpu.VMEM((count, seqs, count), F32),
            pltpu.VMEM((count, seqs, width), BF16),
            pltpu.VMEM((lows, highs, seqs, width), BF16),
            pltpu.VMEM((4, lows, highs, seqs, local_cols), BF16),
            pltpu.VMEM((3, lows, highs, seqs, local_cols), BF16),
            pltpu.VMEM((3, highs, seqs, local_cols), BF16),
            pltpu.VMEM((3, highs, seqs, local_cols), BF16),
            pltpu.VMEM((highs, lows, seqs, local_cols), BF16),
            pltpu.VMEM((lows, seqs, local_cols), BF16),
            pltpu.VMEM((lows, seqs, local_cols), BF16),
            pltpu.VMEM((seqs, local_cols), F32),
            pltpu.VMEM((heads_here, seqs, HEAD), F32),
            pltpu.VMEM((lows, highs, seqs, local_cols), BF16),
            pltpu.VMEM((count, seqs, width), BF16),
            pltpu.VMEM((2 * count, seqs, width), BF16),
            pltpu.VMEM((2, lows, highs, seqs, half), BF16),
            pltpu.VMEM((steps, count * seqs // steps, hidden_cols), F32),
            pltpu.VMEM((steps, count * seqs // steps, hidden_cols), F32),
            pltpu.VMEM((steps, count * seqs // steps, hidden_cols), BF16),
            pltpu.VMEM((3, seqs, half), BF16),
            pltpu.VMEM((chunks, lows, highs, seqs, half // chunks), BF16),
            pltpu.VMEM((chunks, lows, highs, seqs, half // chunks), BF16),
            pltpu.VMEM((chunks - 1, lows, highs, seqs, half // chunks), BF16),
            pltpu.VMEM((chunks - 1, highs, seqs, half // chunks), BF16),
            pltpu.VMEM((chunks - 1, highs, seqs, half // chunks), BF16),
            pltpu.VMEM((highs, lows, seqs, half // chunks), BF16),
            pltpu.VMEM((lows, seqs, half // chunks), BF16),
            pltpu.VMEM((lows, seqs, half // chunks), BF16),
            pltpu.VMEM((2, seqs, half), F32),
            pltpu.SemaphoreType.DMA((12,)),
            pltpu.SemaphoreType.DMA((8,)),
            pltpu.SemaphoreType.DMA((4,)),
            pltpu.SemaphoreType.DMA((4,)),
            pltpu.SemaphoreType.DMA((4,)),
            pltpu.SemaphoreType.DMA((4,)),
            pltpu.SemaphoreType.DMA((2,)),
            pltpu.SemaphoreType.DMA((highs,)),
            pltpu.SemaphoreType.DMA((highs,)),
            pltpu.SemaphoreType.DMA((2,)),
            pltpu.SemaphoreType.DMA((highs,)),
            pltpu.SemaphoreType.DMA((highs,)),
            pltpu.SemaphoreType.DMA,
            pltpu.SemaphoreType.DMA((4,)),
            pltpu.SemaphoreType.DMA((chunks,)),
            pltpu.SemaphoreType.DMA((chunks,)),
            pltpu.SemaphoreType.DMA((chunks,)),
        ],
        compiler_params=pltpu.CompilerParams(collective_id=0, has_side_effects=True),
        name="layer",
    )(
        tokens,
        cosine,
        sine,
        routes.T,
        route_gates.T,
        mix_gain.reshape(1, -1),
        post_gain.reshape(1, -1),
        ffn_gain.reshape(1, -1),
        out_gain.reshape(1, -1),
        prior_state,
        query_weight,
        key_weight,
        value_weight,
        gate_weight,
        out_weight,
        expert_gate,
        expert_up,
        expert_down,
        shared_gate,
        shared_up,
        shared_down,
    )
    decays = lax.dynamic_slice_in_dim(
        decay_table(HEADS), lax.axis_index("tp") * heads_here, heads_here, 0
    )
    new_state = (
        decays[None, :, None, None] * prior_state
        + rot_key[..., :, None] * values[..., None, :]
    )
    return (result, new_state)


def solution(mesh):
    count = mesh.shape["ep"]
    lows = 1
    while lows * lows < count:
        lows *= 2
    highs = count // lows
    return jax.shard_map(
        functools.partial(on_device, lows, highs),
        mesh=mesh,
        in_specs=(
            P("ep", None),
            P("ep"),
            P("ep", "tp", None, None),
            P(),
            P(),
            P(),
            P(),
            P("ep", "tp"),
            P("ep", "tp"),
            P("ep", "tp"),
            P("ep", "tp"),
            P("tp", "ep"),
            P("ep", None),
            P("ep", None),
            P("ep", None, "tp"),
            P("ep", None, "tp"),
            P("ep", "tp", None),
            P(None, "tp"),
            P(None, "tp"),
            P("tp", None),
        ),
        out_specs=(P("ep", None), P("ep", "tp", None, None)),
        check_vma=False,
    )
```
